512 devices in a mesh: sp: 64 (over z, y), fs: 4 (over x), tp: 2 (over core).
Axes of the slice: x: 4, y: 8, z: 8, core: 2. Of those that a mesh axis runs over, the one named last changes fastest.
Arguments:
- tokens: bfloat16 [4, 8192, 2048], P('fs', ('sp', 'tp')), may hold values from -6 to 6
- norm_gain: float32 [2048], replicated, may hold values from 0.1 to 1.9
- gla_query_weight: bfloat16 [2048, 512], P('sp', 'tp'), may hold values from -0.125 to 0.125
- gla_key_weight: bfloat16 [2048, 512], P('sp', 'tp'), may hold values from -0.125 to 0.125
- gla_value_weight: bfloat16 [2048, 1024], P('sp', 'tp'), may hold values from -0.125 to 0.125
- decay_down: bfloat16 [2048, 32], P('sp'), may hold values from -0.125 to 0.125
- decay_up: bfloat16 [32, 512], P(None, 'tp'), may hold values from -1 to 1
- decay_bias: float32 [512], P('tp'), may hold values from 0.5 to 12
- head_gain: float32 [128], replicated, may hold values from 0.1 to 1.9
- window_query_weight: bfloat16 [2048, 1024], P('sp', 'tp'), may hold values from -3 to 3
- window_key_weight: bfloat16 [2048, 256], P('sp', 'tp'), may hold values from -3 to 3
- window_value_weight: bfloat16 [2048, 256], P('sp', 'tp'), may hold values from -0.125 to 0.125
- sink_logit: float32 [16], P('tp'), may hold values from 3 to 7
- gla_output_weight: bfloat16 [1024, 2048], P('tp', 'sp'), may hold values from -0.125 to 0.125
- window_output_weight: bfloat16 [1024, 2048], P('tp', 'sp'), may hold values from -0.125 to 0.125
Outputs:
- mixed: bfloat16 [4, 8192, 2048], P('fs', ('sp', 'tp'))
The draws below stay inside these ranges and needn't reach their ends.
All inputs are finite; a program needn't handle non-finite values.
Results may differ from the reference program's by a relative error of at most 0.013.
Values may be sent and summed in bfloat16 or wider, within the bound.
A program may use at most 64 MiB of HBM per device.

```python
import jax
import jax.numpy as jnp
from jax import lax

D = 2048
GLA_HEADS = 8
KEY_DIM = 64
VALUE_DIM = 128
RANK = 32
SWA_HEADS = 16
KV_HEADS = 4
HEAD_DIM = 64
WINDOW = 128
SPAN = 64
SEQS = 4
LEN = 8192


def gain_values(key):
    normal_draw = jax.random.normal(jax.random.fold_in(key, 11), (D,), jnp.float32)
    return 1.0 + 0.18 * jnp.clip(normal_draw, -5.0, 5.0)


def drawn_weight(key, salt_value, columns):
    raw_draw = jax.random.normal(jax.random.fold_in(key, salt_value), (D, columns), jnp.float32)
    raw_draw = jnp.clip(raw_draw, -6.0, 6.0) / jnp.sqrt(float(D))
    return raw_draw


def draw_window_query_weight(key, part):
    return drawn_weight(key, 16, SWA_HEADS * HEAD_DIM).astype(jnp.bfloat16)


def draw_window_key_weight(key, part):
    return drawn_weight(key, 17, KV_HEADS * HEAD_DIM).astype(jnp.bfloat16)


def draw_norm_gain(key, part):
    return gain_values(key)


def draw_tokens(key, part):
    base_draw = jax.random.normal(jax.random.fold_in(key, 21), (SEQS, LEN, D), jnp.float32)
    base_draw = jnp.clip(base_draw, -6.0, 6.0)
    return base_draw.astype(jnp.bfloat16)


def block_scale(stream_key, extent, split, smallest, high):
    level = 1.0
    for dim, blocks in split:
        steps = jax.random.uniform(jax.random.fold_in(jax.random.fold_in(stream_key, 6), dim), (blocks,), jnp.float32, smallest / len(split), high / len(split))
        level = level * jnp.repeat(jnp.exp(steps), extent[dim] // blocks).reshape((-1,) + (1,) * (len(extent) - 1 - dim))
    return level


def gaussian(own_key, extent, deviation, limit, pieces=(), held_as=jnp.bfloat16):
    values = deviation * jax.random.normal(own_key, extent, jnp.float32)
    if pieces:
        values = values * block_scale(own_key, extent, pieces, -0.22, 0.18)
    return jnp.clip(values, -limit, limit).astype(held_as)


def setup_inputs(seed: int = 0) -> dict:
    streams_of = jax.random.split(jax.random.key(seed), 16)
    tokens = draw_tokens(jax.random.fold_in(streams_of[15], 71), 0)
    norm_gain = draw_norm_gain(jax.random.fold_in(streams_of[15], 71), 0)
    gla_query_weight = gaussian(streams_of[2], (D, GLA_HEADS * KEY_DIM), D ** -0.5, 0.125, ((0, 64), (1, 2)))
    gla_key_weight = gaussian(streams_of[3], (D, GLA_HEADS * KEY_DIM), D ** -0.5, 0.125, ((0, 64), (1, 2)))
    gla_value_weight = gaussian(streams_of[4], (D, GLA_HEADS * VALUE_DIM), D ** -0.5, 0.125, ((0, 64), (1, 2)))
    decay_down = gaussian(streams_of[5], (D, RANK), D ** -0.5, 0.125, ((0, 64),))
    decay_up = gaussian(streams_of[6], (RANK, GLA_HEADS * KEY_DIM), RANK ** -0.5, 1.0, ((1, 2),))
    decay_bias = jnp.clip(0.5 + 11.5 * jax.random.uniform(streams_of[7], (GLA_HEADS * KEY_DIM,), jnp.float32) ** block_scale(streams_of[7], (GLA_HEADS * KEY_DIM,), ((0, 2),), -0.2, 0.2), 0.5, 12.0)
    head_gain = jnp.clip(1.0 + 0.18 * jax.random.normal(streams_of[8], (VALUE_DIM,), jnp.float32), 0.1, 1.9)
    window_query_weight = draw_window_query_weight(jax.random.fold_in(streams_of[15], 71), 0)
    window_key_weight = draw_window_key_weight(jax.random.fold_in(streams_of[15], 71), 0)
    window_value_weight = gaussian(streams_of[11], (D, KV_HEADS * HEAD_DIM), D ** -0.5, 0.125, ((0, 64), (1, 2)))
    sink_logit = jnp.clip(3.0 + 4.0 * jax.random.uniform(streams_of[12], (SWA_HEADS,), jnp.float32) ** block_scale(streams_of[12], (SWA_HEADS,), ((0, 2),), -0.2, 0.2), 3.0, 7.0)
    gla_output_weight = gaussian(streams_of[13], (GLA_HEADS * VALUE_DIM, D), (GLA_HEADS * VALUE_DIM + SWA_HEADS * HEAD_DIM) ** -0.5, 0.125, ((0, 2), (1, 64)))
    window_output_weight = gaussian(streams_of[14], (SWA_HEADS * HEAD_DIM, D), (GLA_HEADS * VALUE_DIM + SWA_HEADS * HEAD_DIM) ** -0.5, 0.125, ((0, 2), (1, 64)))
    return {"tokens": tokens, "norm_gain": norm_gain, "gla_query_weight": gla_query_weight, "gla_key_weight": gla_key_weight, "gla_value_weight": gla_value_weight, "decay_down": decay_down, "decay_up": decay_up, "decay_bias": decay_bias, "head_gain": head_gain, "window_query_weight": window_query_weight, "window_key_weight": window_key_weight, "window_value_weight": window_value_weight, "sink_logit": sink_logit, "gla_output_weight": gla_output_weight, "window_output_weight": window_output_weight}


EPS = 1e-06
SOFTMAX_TEMPER = 16.0
HIGH = lax.Precision.HIGHEST

def rms_rows(values, gain):
    mean_square = lax.optimization_barrier(jnp.mean(values * values, axis=-1, keepdims=True))
    return values * lax.rsqrt(mean_square + EPS) * gain

def block_terms(query_rows, key_rows, value_rows, log_decay_rate, block_len):
    seq_len, head_count, key_width = query_rows.shape
    value_width = value_rows.shape[-1]
    block_count = seq_len // block_len
    q_scaled = query_rows.reshape(block_count, block_len, head_count, key_width) * key_width ** (-0.5)
    k_blocks = key_rows.reshape(block_count, block_len, head_count, key_width)
    v_blocks = value_rows.reshape(block_count, block_len, head_count, value_width)
    within = jnp.cumsum(log_decay_rate.reshape(block_count, block_len, head_count, key_width), axis=1)
    block_total = within[:, -1]
    q_dec = q_scaled * jnp.exp(within)
    k_dec = k_blocks * jnp.exp(-within)
    k_end = k_blocks * jnp.exp(block_total[:, None] - within)
    causal = jnp.tril(jnp.ones((block_len, block_len), dtype=bool))
    scores = jnp.einsum('nihd,njhd->nhij', q_dec, k_dec, precision=HIGH)
    scores = jnp.where(causal, scores, 0.0)
    local_out = jnp.einsum('nhij,njhe->nihe', scores, v_blocks, precision=HIGH)
    update = jnp.einsum('njhd,njhe->nhde', k_end, v_blocks, precision=HIGH)

    def advance(carried, inputs):
        update_in, decay_in = inputs
        return (decay_in[..., None] * carried + update_in, carried)
    start_state = jnp.zeros((head_count, key_width, value_width), jnp.float32)
    last_state, entering = lax.scan(advance, start_state, (update, jnp.exp(block_total)))
    return (q_dec, local_out, entering, last_state, block_total)

def window_band_mask(block_count, block_len, offset):
    query_pos = jnp.arange(block_len)[:, None] + block_len
    key_pos = jnp.arange(2 * block_len)[None, :]
    distance = query_pos - key_pos
    inside = (distance >= 0) & (distance < block_len)
    global_key = offset + jnp.arange(block_count)[:, None, None] * block_len - block_len + key_pos[None]
    return inside[None] & (global_key >= 0)

def window_attend(query_blocks, key_band, value_band, valid, sinks):
    scores = jnp.einsum('nqhgd,nkhd->nhgqk', query_blocks.astype(jnp.float32), key_band.astype(jnp.float32))
    scores = scores * HEAD_DIM ** (-0.5)
    scores = jnp.where(valid[:, None, None], scores, -1e+30)
    sink_term = sinks[None, :, :, None, None]
    top = jnp.maximum(lax.optimization_barrier(jnp.max(scores, axis=-1, keepdims=True)), sink_term)
    expo = jnp.exp(scores - top)
    denom = lax.optimization_barrier(jnp.sum(expo, axis=-1, keepdims=True)) + jnp.exp(sink_term - top)
    weights = (expo / denom).astype(jnp.bfloat16)
    attended = jnp.einsum('nhgqk,nkhd->nqhgd', weights.astype(jnp.float32), value_band.astype(jnp.float32))
    return attended.astype(jnp.bfloat16)

def reference(tokens, norm_gain, gla_query_weight, gla_key_weight, gla_value_weight, decay_down, decay_up, decay_bias, head_gain, window_query_weight, window_key_weight, window_value_weight, sink_logit, gla_output_weight, window_output_weight):

    def one_sequence(seq_rows):
        seq_len = seq_rows.shape[0]
        normed = rms_rows(seq_rows.astype(jnp.float32), norm_gain).astype(jnp.bfloat16)

        def project(weight):
            return jnp.dot(normed, weight, preferred_element_type=jnp.float32).astype(jnp.bfloat16)
        gla_query = project(gla_query_weight)
        gla_key = project(gla_key_weight)
        gla_value = project(gla_value_weight)
        low_rank = project(decay_down)
        gate_logit_values = jnp.dot(low_rank, decay_up, preferred_element_type=jnp.float32) + decay_bias
        log_decay_rate = jax.nn.log_sigmoid(gate_logit_values) / SOFTMAX_TEMPER
        q_dec, local_out, entering, last_state, block_total = block_terms(gla_query.astype(jnp.float32).reshape(seq_len, GLA_HEADS, KEY_DIM), gla_key.astype(jnp.float32).reshape(seq_len, GLA_HEADS, KEY_DIM), gla_value.astype(jnp.float32).reshape(seq_len, GLA_HEADS, VALUE_DIM), log_decay_rate.reshape(seq_len, GLA_HEADS, KEY_DIM), SPAN)
        gla_out = local_out + jnp.einsum('nihd,nhde->nihe', q_dec, entering, precision=HIGH)
        gla_out = gla_out.reshape(seq_len, GLA_HEADS, VALUE_DIM)
        gla_hidden = rms_rows(gla_out, head_gain).astype(jnp.bfloat16).reshape(seq_len, GLA_HEADS * VALUE_DIM)
        window_query = project(window_query_weight)
        sliding_key = project(window_key_weight)
        window_value = project(window_value_weight)
        block_count = seq_len // WINDOW
        group_size = SWA_HEADS // KV_HEADS
        query_blocks = window_query.reshape(block_count, WINDOW, KV_HEADS, group_size, HEAD_DIM)

        def banded(rows):
            blocks = rows.reshape(block_count, WINDOW, KV_HEADS, HEAD_DIM)
            earlier = jnp.concatenate([jnp.zeros_like(blocks[:1]), blocks[:-1]], axis=0)
            return jnp.concatenate([earlier, blocks], axis=1)
        valid = window_band_mask(block_count, WINDOW, 0)
        sinks = sink_logit.reshape(KV_HEADS, group_size)
        window_hidden = window_attend(query_blocks, banded(sliding_key), banded(window_value), valid, sinks)
        window_hidden = window_hidden.reshape(seq_len, SWA_HEADS * HEAD_DIM)
        total = jnp.dot(gla_hidden, gla_output_weight, preferred_element_type=jnp.float32)
        total = total + jnp.dot(window_hidden, window_output_weight, preferred_element_type=jnp.float32)
        return total.astype(jnp.bfloat16)
    return lax.map(one_sequence, tokens)
```

```python
import jax
import jax.numpy as jnp
from jax import lax
from jax.sharding import Mesh
from jax.sharding import PartitionSpec as P

KEY_DIM = 64
VALUE_DIM = 128
HEAD_DIM = 64
WINDOW = 128
SPAN = 64
SP = ("sp_0", "sp_1")
SP_TP = ("sp_0", "sp_1", "tp")
GROUP = ("fs", "tp")
EPS = 1e-06
SOFTMAX_TEMPER = 16.0
HIGH = lax.Precision.HIGHEST


def rms_rows(values, gain):
    mean_square = jnp.mean(values * values, axis=-1, keepdims=True)
    return values * lax.rsqrt(mean_square + EPS) * gain


def own_part(value, at, size, dim):
    return lax.dynamic_slice_in_dim(value, at * size, size, axis=dim)


def combine(earlier, later):
    return (later[1][..., None] * earlier[0] + later[0], earlier[1] * later[1])


def carried_in(value):
    start = (jnp.zeros_like(value[0]), jnp.ones_like(value[1]))
    before, subtotal = start, value
    for axis in ("sp_1", "sp_0"):
        peers, place = lax.axis_size(axis), lax.axis_index(axis)
        both = jnp.concatenate(
            [subtotal[0], jnp.broadcast_to(subtotal[1][..., None], subtotal[0].shape[:-1] + (1,))], -1
        )
        pieces = lax.all_gather(both, axis)
        inside, subtotal = start, start
        for k in range(peers):
            subtotal = combine(subtotal, (pieces[k, ..., :-1], pieces[k, ..., -1]))
            inside = jax.tree.map(lambda n, o: jnp.where(k < place, n, o), subtotal, inside)
        before = combine(inside, before)
    return before[0]


def per_device(
    tokens, norm_gain, gla_query_weight, gla_key_weight, gla_value_weight, decay_down, decay_up,
    decay_bias, head_gain, window_query_weight, window_key_weight, window_value_weight, sink_logit,
    gla_output_weight, window_output_weight,
):
    x = lax.axis_index("fs")
    rows = lax.all_gather(tokens[0], GROUP, axis=0, tiled=True)
    w_in = jnp.concatenate(
        [
            own_part(gla_query_weight, x, 64, 1),
            own_part(gla_key_weight, x, 64, 1),
            own_part(gla_value_weight, x, 128, 1),
            own_part(window_query_weight, x, 128, 1),
            own_part(window_key_weight, x // 2, 64, 1),
            own_part(window_value_weight, x // 2, 64, 1),
            decay_down,
        ],
        axis=1,
    )
    w_in = lax.all_gather(w_in, SP, axis=0, tiled=True)
    w_out = jnp.concatenate(
        [own_part(gla_output_weight, x, 128, 0), own_part(window_output_weight, x, 128, 0)], axis=0
    ).T
    w_out = lax.all_gather(w_out, SP, axis=0, tiled=True)
    normed = rms_rows(rows.astype(jnp.float32), norm_gain).astype(jnp.bfloat16)
    proj = jnp.dot(normed, w_in, preferred_element_type=jnp.float32).astype(jnp.bfloat16)
    seqs = 4
    spans = rows.shape[0] // seqs // SPAN
    gate = jnp.dot(proj[:, 512:], own_part(decay_up, x, 64, 1), preferred_element_type=jnp.float32)
    log_rate = jax.nn.log_sigmoid(gate + own_part(decay_bias, x, 64, 0)) / SOFTMAX_TEMPER

    def blocks(v):
        return v.astype(jnp.float32).reshape(seqs, spans, SPAN, -1)

    q, k, v = blocks(proj[:, :64]) * KEY_DIM**-0.5, blocks(proj[:, 64:128]), blocks(proj[:, 128:256])
    within = jnp.cumsum(blocks(log_rate), axis=2)
    block_total = within[:, :, -1]
    q_dec = q * jnp.exp(within)
    k_dec = k * jnp.exp(-within)
    k_end = k * jnp.exp(block_total[:, :, None] - within)
    scores = jnp.einsum("snid,snjd->snij", q_dec, k_dec, precision=HIGH)
    scores = jnp.where(jnp.tril(jnp.ones((SPAN, SPAN), bool)), scores, 0.0)
    local_out = jnp.einsum("snij,snje->snie", scores, v, precision=HIGH)
    update = jnp.einsum("snjd,snje->snde", k_end, v, precision=HIGH)
    decay = jnp.exp(block_total)
    last_state = decay[:, 1, :, None] * update[:, 0] + update[:, 1]
    incoming = carried_in((last_state, decay[:, 0] * decay[:, 1]))
    entering = jnp.stack([incoming, decay[:, 0, :, None] * incoming + update[:, 0]], axis=1)

    wq = proj[:, 256:384].reshape(seqs, WINDOW, 2, HEAD_DIM)
    wkv = proj[:, 384:512].reshape(seqs, WINDOW, 2 * HEAD_DIM)
    ny, nz = lax.axis_size("sp_1"), lax.axis_size("sp_0")
    n = ny * nz
    edge = lax.ppermute(wkv, SP, [(i, i + 1) for i in range(n - 1)])
    band = jnp.concatenate([edge, wkv], axis=1)
    s = jnp.einsum("sqhd,skd->shqk", wq, band[..., :64], preferred_element_type=jnp.float32)
    s = s * HEAD_DIM**-0.5
    dist = jnp.arange(WINDOW)[:, None] + WINDOW - jnp.arange(2 * WINDOW)[None]
    ok = (dist >= 0) & (dist < WINDOW)
    ok = ok & ((lax.axis_index(SP) > 0) | (jnp.arange(2 * WINDOW)[None] >= WINDOW))
    s = jnp.where(ok, s, -1e30)
    sink = own_part(sink_logit, x, 2, 0)[None, :, None, None]
    top = jnp.maximum(jnp.max(s, -1, keepdims=True), sink)
    e = jnp.exp(s - top)
    den = jnp.sum(e, -1, keepdims=True) + jnp.exp(sink - top)
    att = jnp.einsum(
        "shqk,skd->sqhd", (e / den).astype(jnp.bfloat16), band[..., 64:],
        preferred_element_type=jnp.float32,
    ).astype(jnp.bfloat16)

    gla_out = local_out + jnp.einsum("snid,snde->snie", q_dec, entering, precision=HIGH)
    hidden = rms_rows(gla_out, head_gain).astype(jnp.bfloat16).reshape(-1, VALUE_DIM)
    hidden = jnp.concatenate([hidden, att.reshape(-1, 128)], axis=1)
    total = jnp.einsum("rk,nk->rn", hidden, w_out, preferred_element_type=jnp.float32)
    total = total.astype(jnp.bfloat16).reshape(8, -1, total.shape[1])
    arrived = lax.all_to_all(total, GROUP, split_axis=0, concat_axis=0, tiled=True)
    return arrived.astype(jnp.float32).sum(axis=0).astype(jnp.bfloat16)[None]


def solution(mesh):
    split = Mesh(
        mesh.devices.reshape(8, 8, mesh.shape["fs"], mesh.shape["tp"]), ("sp_0", "sp_1", "fs", "tp")
    )
    return jax.shard_map(
        per_device,
        mesh=split,
        in_specs=(
            P("fs", SP_TP, None), P(), P(SP, "tp"), P(SP, "tp"), P(SP, "tp"), P(SP, None),
            P(None, "tp"), P("tp"), P(), P(SP, "tp"), P(SP, "tp"), P(SP, "tp"), P("tp"),
            P("tp", SP), P("tp", SP),
        ),
        out_specs=P("fs", SP_TP, None),
        check_vma=False,
    )
```

```python
import functools

import jax
import jax.numpy as jnp
from jax import lax
from jax.experimental import pallas as pl
from jax.experimental.pallas import tpu as pltpu
from jax.sharding import Mesh
from jax.sharding import PartitionSpec as P

F32, BF16 = jnp.float32, jnp.bfloat16
MESH = pl.DeviceIdType.MESH
HIGH = lax.Precision.HIGHEST
SP = ("sp_0", "sp_1")
SP_TP = ("sp_0", "sp_1", "tp")
EPS = 1e-06
N = 8
SEQS = 4
D = 2048
PARTS = ((0, 5, "sp_1", "sp_0"), (5, 9, "sp_0", "sp_1"), (9, 11, "sp_1", "sp_0"), (11, 13, "sp_0", "sp_1"))


def dot(a, b, contract=((1,), (0,)), precision=None):
    return lax.dot_general(
        a, b, (contract, ((), ())), precision=precision, preferred_element_type=F32
    )


def wrap(i, n=N):
    return lax.rem(i + 4 * n, n)


def kernel(
    tokens, norm_gain, gq, gk, gv, decay_down, decay_up, decay_bias, head_gain, wq, wk, wv,
    sink, go, wo, out,
    W, T, normed, kv, edge, state, got1, tot, got2, ret, enter, take, hop, hopin, fin, finin,
    w_send, w_recv, t_send, t_recv, p_send, p_recv, e_sem, s_send, s_recv, o_send, o_recv,
    x_send, x_recv,
):
    z, y = lax.axis_index("sp_0"), lax.axis_index("sp_1")
    x, c = lax.axis_index("fs"), lax.axis_index("tp")
    me = z * N + y
    at = {"sp_0": z, "sp_1": y}
    right, left, across = wrap(x + 1, 4), wrap(x - 1, 4), wrap(x + 2, 4)
    partner = {"tp": 1 - c}
    after, before = wrap(me + 1, 64), wrap(me - 1, 64)
    after_id = {"sp_0": after // N, "sp_1": lax.rem(after, N)}
    before_id = {"sp_0": before // N, "sp_1": lax.rem(before, N)}

    barrier = pltpu.get_barrier_semaphore()

    def greet(device_id):
        pl.semaphore_signal(barrier, inc=1, device_id=device_id, device_id_type=MESH)

    for name in SP:
        for d in range(1, N):
            greet({name: wrap(at[name] + d)})
    greet({"fs": right})
    greet({"fs": left})
    greet(partner)
    greet(after_id)
    greet(before_id)

    def pick(ref, width, index, count):
        got = ref[:, 0:width]
        for i in range(1, count):
            got = jnp.where(index == i, ref[:, i * width : (i + 1) * width], got)
        return got

    def put(block, value):
        W[me, block] = value[0:16]
        W[me, block + 1] = value[16:32]

    put(0, jnp.concatenate([pick(gq, 64, x, 4), pick(gk, 64, x, 4)], axis=1))
    put(2, pick(gv, 128, x, 4))
    down = decay_down[...]
    W[me, 4] = jnp.concatenate([down[0:16], down[16:32], jnp.zeros((16, 64), BF16)], axis=1)
    put(5, pick(wq, 128, x, 4))
    put(7, jnp.concatenate([pick(wk, 64, x // 2, 2), pick(wv, 64, x // 2, 2)], axis=1))
    eye = (
        lax.broadcasted_iota(jnp.int32, (32, 32), 0) == lax.broadcasted_iota(jnp.int32, (32, 32), 1)
    ).astype(BF16)
    own_rows = pl.ds(pl.multiple_of(x * 128, 128), 128)
    put(9, dot(eye, go[own_rows, :], ((1,), (1,))).astype(BF16))
    put(11, dot(eye, wo[own_rows, :], ((1,), (1,))).astype(BF16))
    for q in range(4):
        T[x, c, q] = tokens[q]

    pl.semaphore_wait(barrier, 2 * (N - 1) + 5)

    def piece(part, shard, device_id):
        a, b, _, _ = PARTS[part]
        ref = W.at[shard, a:b]
        return pltpu.make_async_remote_copy(
            src_ref=ref, dst_ref=ref, send_sem=w_send.at[part], recv_sem=w_recv.at[part, shard],
            device_id=device_id, device_id_type=MESH,
        )

    def first_hop(part):
        name = PARTS[part][2]
        for d in (1, 7, 2, 6, 3, 5, 4):
            piece(part, me, {name: wrap(at[name] + d)}).start()

    def ring_step(part, h, j):
        _, _, near, far = PARTS[part]
        offset = ((j + 1) // 2) * (2 * lax.rem(j, 2) - 1)
        line = wrap(at[near] + offset)
        up, down_ = {far: wrap(at[far] + 1)}, {far: wrap(at[far] - 1)}

        def shard(across_by):
            spot = wrap(at[far] + across_by)
            return line * N + spot if near == "sp_0" else spot * N + line

        def arrive(s):
            piece(part, s, up).wait_recv()

        if h == 0:
            s = shard(0)
            pl.when(j > 0)(lambda: arrive(s))
            piece(part, s, up).start()
            piece(part, s, down_).start()
        elif h < 3:
            s = shard(-h)
            arrive(s)
            piece(part, s, up).start()
            s = shard(h)
            arrive(s)
            piece(part, s, down_).start()
        elif h == 3:
            s, r = shard(-3), shard(3)
            arrive(s)
            pl.when(j < 4)(lambda: piece(part, s, up).start())
            arrive(r)
            pl.when(j >= 4)(lambda: piece(part, r, down_).start())
        else:
            arrive(shard(4))

    def ring(parts, h, more=None):
        def body(j, carry):
            for part in parts:
                ring_step(part, h, j)
            if more is not None:
                more(j)
            return carry

        lax.fori_loop(0, N, body, 0)

    def chunk(seq, q, device_id, own=False):
        return pltpu.make_async_remote_copy(
            src_ref=tokens.at[q] if own else T.at[seq, c, q], dst_ref=T.at[seq, c, q],
            send_sem=t_send, recv_sem=t_recv.at[seq, q], device_id=device_id, device_id_type=MESH,
        )

    def twin(seq, q, own=False):
        return pltpu.make_async_remote_copy(
            src_ref=tokens.at[q] if own else T.at[seq, c, q], dst_ref=T.at[seq, c, q],
            send_sem=p_send, recv_sem=p_recv.at[seq, q], device_id=partner, device_id_type=MESH,
        )

    def tokens_step(i):
        if i < 4:
            arrivals = ((left, i, right), (right, (i + 2) % 4, left))
        else:
            arrivals = ((across, i - 4, None), (across, i - 2, None))
        for seq, q, onward in arrivals:
            chunk(seq, q, partner).wait_recv()
            if i < 2:
                chunk(seq, q, {"fs": onward}).start()
            twin(seq, q).start()

    for i in range(4):
        chunk(x, i, {"fs": right}, True).start()
        chunk(x, (i + 2) % 4, {"fs": left}, True).start()
    first_hop(0)
    first_hop(1)
    for q in range(4):
        twin(x, q, True).start()
    first_hop(2)
    first_hop(3)
    tokens_step(0)
    tokens_step(1)
    ring((0, 1), 0)
    tokens_step(2)
    tokens_step(3)
    ring((0, 1), 1)
    tokens_step(4)
    tokens_step(5)
    for seq in range(SEQS):
        for q in range(4):
            pltpu.make_async_remote_copy(
                src_ref=T.at[seq, 1 - c, q], dst_ref=T.at[seq, 1 - c, q], send_sem=p_send,
                recv_sem=p_recv.at[seq, q], device_id=partner, device_id_type=MESH,
            ).wait_recv()

    def norm_rows(j, offset):
        index = 2 * j + offset
        seq, half = index // 8, lax.rem(index // 4, 2)
        q = lax.rem(index, 4)
        rows = T[seq, half, q].astype(F32)
        mean_square = jnp.mean(rows * rows, axis=-1, keepdims=True)
        rows = rows * lax.rsqrt(mean_square + EPS) * norm_gain[...]
        normed[pl.ds(pl.multiple_of(index * 16, 16), 16), :] = rows.astype(BF16)

    def norm_two(base):
        def more(j):
            norm_rows(j, base)
            norm_rows(j, base + 1)

        return more

    ring((0, 1), 2, norm_two(0))
    ring((0, 1), 3, norm_two(16))
    ring((0,), 4)

    def tile(block):
        return W[:, block : block + 2].reshape(D, 128)

    rows = normed[...]
    lane = lax.broadcasted_iota(jnp.int32, (64, 16, 128), 2)
    low = W[:, 4]
    zero = jnp.zeros_like(low)
    low = jnp.stack([jnp.where(lane < 32, low, zero), jnp.where(lane >= 32, low, zero)], axis=1)
    low = dot(rows, low.reshape(D, 128))
    low_rank = (low[:, 0:32] + low[:, 32:64]).astype(BF16)
    proj = dot(rows, jnp.concatenate([tile(0), tile(2)], axis=1))
    gate = dot(low_rank, pick(decay_up, 64, x, 4)) + pick(decay_bias, 64, x, 4)
    u = jnp.exp(-jnp.abs(gate))
    log1p = jnp.where(u < 0.01, u * (1.0 - u * (0.5 - u * (1.0 / 3.0))), jnp.log(1.0 + u))
    log_rate = (jnp.minimum(gate, 0.0) - log1p) / 16.0
    query = proj[:, 0:64].astype(BF16).astype(F32) * 64**-0.5
    key = proj[:, 64:128].astype(BF16).astype(F32)
    value = proj[:, 128:256].astype(BF16).astype(F32)

    lower = lax.broadcasted_iota(jnp.int32, (64, 64), 0) >= lax.broadcasted_iota(jnp.int32, (64, 64), 1)
    ones = lower.astype(F32)
    spans = [slice(64 * i, 64 * (i + 1)) for i in range(2 * SEQS)]
    within = [dot(ones, log_rate[r], precision=HIGH) for r in spans]
    totals = [w[63:64] for w in within]
    column = [jnp.transpose(jnp.broadcast_to(t, (128, 64))) for t in totals]
    update = [
        dot(jnp.transpose(key[r] * jnp.exp(t - w)), value[r], precision=HIGH)
        for r, w, t in zip(spans, within, totals)
    ]
    for seq in range(SEQS):
        a, b = 2 * seq, 2 * seq + 1
        last = jnp.exp(column[b]) * update[a] + update[b]
        fall = column[a] + column[b]
        for half in range(2):
            part = slice(32 * half, 32 * (half + 1))
            state[a + half, 0] = last[part].astype(BF16)
            state[a + half, 1] = fall[part].astype(BF16)

    def spread(stage, name, src, dst):
        place = at[name]
        for d in (4, 3, 5, 2, 6, 1, 7):
            peer = wrap(place + d)
            pltpu.make_async_remote_copy(
                src_ref=src(peer), dst_ref=dst.at[place], send_sem=s_send.at[stage, d],
                recv_sem=s_recv.at[stage, place], device_id={name: peer}, device_id_type=MESH,
            ).start()

    def spread_wait(stage, name, src, dst):
        place = at[name]
        for d in (1, 7, 2, 6, 3, 5, 4):
            peer = wrap(place + d)
            pltpu.make_async_remote_copy(
                src_ref=src(peer), dst_ref=dst.at[peer], send_sem=s_send.at[stage, d],
                recv_sem=s_recv.at[stage, peer], device_id={name: peer}, device_id_type=MESH,
            ).wait()

    spread(0, "sp_1", lambda i: state.at[i], got1)
    got1[y] = state[y]

    ring((1,), 4)
    wproj = dot(rows, jnp.concatenate([tile(5), tile(7)], axis=1)).astype(BF16)
    for seq in range(SEQS):
        kv[seq] = wproj[128 * seq : 128 * (seq + 1), 128:256]

    q_dec = [query[r] * jnp.exp(w) for r, w in zip(spans, within)]
    edge_copy = pltpu.make_async_remote_copy(
        src_ref=kv, dst_ref=edge, send_sem=e_sem.at[0], recv_sem=e_sem.at[1],
        device_id=after_id, device_id_type=MESH,
    )
    edge_copy.start()

    local = []
    for r, w, qd in zip(spans, within, q_dec):
        scores = dot(qd, key[r] * jnp.exp(-w), ((1,), (1,)), HIGH)
        local.append(dot(jnp.where(lower, scores, 0.0), value[r], precision=HIGH))

    spread_wait(0, "sp_1", lambda i: state.at[i], got1)
    run = jnp.zeros((32, 128), F32)
    fall = jnp.zeros((32, 128), F32)
    prefix, falls = [], []
    for i in range(N):
        prefix.append(run)
        falls.append(fall)
        step = got1[i, 1].astype(F32)
        run = jnp.exp(step) * run + got1[i, 0].astype(F32)
        fall = fall + step
    tot[0] = run.astype(BF16)
    tot[1] = fall.astype(BF16)
    spread(1, "sp_0", lambda i: tot, got2)
    got2[z] = tot[...]

    ring((2, 3), 0)
    ring((2, 3), 1)
    spread_wait(1, "sp_0", lambda i: tot, got2)
    come = jnp.zeros((32, 128), F32)
    for i in range(N):
        come = jnp.where(
            i < z, jnp.exp(got2[i, 1].astype(F32)) * come + got2[i, 0].astype(F32), come
        )
    for i in range(N):
        ret[i] = (jnp.exp(falls[i]) * come + prefix[i]).astype(BF16)
    spread(2, "sp_1", lambda i: ret.at[i], enter)
    enter[y] = ret[y]

    ring((2, 3), 2)
    edge_copy.wait()
    distance = (
        lax.broadcasted_iota(jnp.int32, (128, 256), 0)
        + 128
        - lax.broadcasted_iota(jnp.int32, (128, 256), 1)
    )
    first_key = jnp.where(me > 0, 0, 128)
    valid = (distance >= 0) & (distance < 128)
    valid = valid & (lax.broadcasted_iota(jnp.int32, (128, 256), 1) >= first_key)
    sinks = pick(sink, 2, x, 4)
    window = []
    for seq in range(SEQS):
        band = jnp.concatenate([edge[seq], kv[seq]], axis=0)
        heads = []
        for head in range(2):
            qh = wproj[128 * seq : 128 * (seq + 1), 64 * head : 64 * (head + 1)]
            s = dot(qh, band[:, 0:64], ((1,), (1,))) * 64**-0.5
            s = jnp.where(valid, s, -1e30)
            sink_term = sinks[:, head : head + 1]
            top = jnp.maximum(jnp.max(s, axis=-1, keepdims=True), sink_term)
            expo = jnp.exp(s - top)
            denom = jnp.sum(expo, axis=-1, keepdims=True) + jnp.exp(sink_term - top)
            heads.append(dot((expo / denom).astype(BF16), band[:, 64:128]))
        window.append(jnp.concatenate(heads, axis=1).astype(BF16))
        if seq == 1:
            ring((2, 3), 3)
    ring((2, 3), 4)

    spread_wait(2, "sp_1", lambda i: ret.at[i], enter)
    hidden = []
    for seq in range(SEQS):
        a, b = 2 * seq, 2 * seq + 1
        come = jnp.concatenate([enter[a], enter[b]], axis=0).astype(F32)
        middle = jnp.exp(column[a]) * come + update[a]
        for i, entering in ((a, come), (b, middle)):
            gla = local[i] + dot(q_dec[i], entering, precision=HIGH)
            mean_square = jnp.mean(gla * gla, axis=-1, keepdims=True)
            hidden.append((gla * lax.rsqrt(mean_square + EPS) * head_gain[...]).astype(BF16))

    out_map = jnp.concatenate([tile(9), tile(11)], axis=1)

    def total(seq_static):
        h = jnp.concatenate(hidden[2 * seq_static : 2 * seq_static + 2], axis=0)
        return dot(jnp.concatenate([h, window[seq_static]], axis=1), out_map, ((1,), (1,)))

    for seq in range(SEQS):
        t = total(seq)
        normed[128 * seq : 128 * (seq + 1), :] = t.astype(BF16)

    def to_partner(seq):
        return pltpu.make_async_remote_copy(
            src_ref=normed.at[pl.ds(pl.multiple_of(seq * 128 + (1 - c) * 64, 64), 64), :],
            dst_ref=take.at[seq], send_sem=o_send.at[seq], recv_sem=o_recv.at[seq],
            device_id=partner, device_id_type=MESH,
        )

    for seq in (across, right, left, x):
        to_partner(seq).start()

    def chip_sum(seq):
        to_partner(seq).wait_recv()
        own = normed[pl.ds(pl.multiple_of(seq * 128 + c * 64, 64), 64), :]
        return own.astype(F32) + take[seq].astype(F32)

    def move(index, src, dst, device_id):
        return pltpu.make_async_remote_copy(
            src_ref=src, dst_ref=dst, send_sem=x_send.at[index], recv_sem=x_recv.at[index],
            device_id={"fs": device_id}, device_id_type=MESH,
        )

    s = chip_sum(across).astype(BF16)
    hop[0] = s[:, 0:1024]
    hop[1] = s[:, 1024:2048]
    moves = [move(0, hop.at[0], hopin.at[0], right), move(1, hop.at[1], hopin.at[1], left)]
    moves[0].start()
    moves[1].start()
    to_right = chip_sum(right)
    fin[1] = to_right[:, 1024:2048].astype(BF16)
    moves.append(move(2, fin.at[1], finin.at[1], right))
    moves[2].start()
    to_left = chip_sum(left)
    fin[2] = to_left[:, 0:1024].astype(BF16)
    moves.append(move(3, fin.at[2], finin.at[2], left))
    moves[3].start()
    moves[0].wait_recv()
    fin[0] = (to_right[:, 0:1024] + hopin[0].astype(F32)).astype(BF16)
    moves.append(move(4, fin.at[0], finin.at[0], right))
    moves[4].start()
    moves[1].wait_recv()
    fin[3] = (to_left[:, 1024:2048] + hopin[1].astype(F32)).astype(BF16)
    moves.append(move(5, fin.at[3], finin.at[3], left))
    moves[5].start()
    mine = chip_sum(x)
    for i in (2, 3, 4, 5):
        moves[i].wait_recv()
    low_half = mine[:, 0:1024] + finin[0].astype(F32) + finin[2].astype(F32)
    high_half = mine[:, 1024:2048] + finin[1].astype(F32) + finin[3].astype(F32)
    out[:, 0:1024] = low_half.astype(BF16)
    out[:, 1024:2048] = high_half.astype(BF16)

    for i in range(6):
        moves[i].wait_send()
    for seq in range(SEQS):
        to_partner(seq).wait_send()
    for part in range(4):
        a, b, _, _ = PARTS[part]
        ref = W.at[0:63, a:b]
        pltpu.make_async_copy(ref, ref, w_send.at[part]).wait()
    ref = T.at[0:3, 0]
    pltpu.make_async_copy(ref, ref, t_send).wait()
    ref = T.at[0:4, 0]
    pltpu.make_async_copy(ref, ref, p_send).wait()


def per_device(
    tokens, norm_gain, gla_query_weight, gla_key_weight, gla_value_weight, decay_down, decay_up,
    decay_bias, head_gain, window_query_weight, window_key_weight, window_value_weight, sink_logit,
    gla_output_weight, window_output_weight,
):
    dma, vmem = pltpu.SemaphoreType.DMA, pltpu.VMEM
    return pl.pallas_call(
        kernel,
        out_shape=jax.ShapeDtypeStruct((64, D), BF16),
        in_specs=[pl.BlockSpec(memory_space=pltpu.VMEM)] * 15,
        out_specs=pl.BlockSpec(memory_space=pltpu.VMEM),
        scratch_shapes=[
            vmem((64, 13, 16, 128), BF16),
            vmem((4, 2, 4, 16, D), BF16),
            vmem((512, D), BF16),
            vmem((4, 128, 128), BF16),
            vmem((4, 128, 128), BF16),
            vmem((N, 2, 32, 128), BF16),
            vmem((N, 2, 32, 128), BF16),
            vmem((2, 32, 128), BF16),
            vmem((N, 2, 32, 128), BF16),
            vmem((N, 32, 128), BF16),
            vmem((N, 32, 128), BF16),
            vmem((4, 64, D), BF16),
            vmem((2, 64, 1024), BF16),
            vmem((2, 64, 1024), BF16),
            vmem((4, 64, 1024), BF16),
            vmem((4, 64, 1024), BF16),
            dma((4,)),
            dma((4, 64)),
            dma,
            dma((4, 4)),
            dma,
            dma((4, 4)),
            dma((2,)),
            dma((3, N)),
            dma((3, N)),
            dma((4,)),
            dma((4,)),
            dma((6,)),
            dma((6,)),
        ],
        compiler_params=pltpu.CompilerParams(
            collective_id=0, has_side_effects=True, vmem_limit_bytes=48 * 1024 * 1024
        ),
    )(
        tokens.reshape(4, 16, D),
        norm_gain.reshape(1, D),
        gla_query_weight,
        gla_key_weight,
        gla_value_weight,
        decay_down,
        decay_up,
        decay_bias.reshape(1, -1),
        head_gain.reshape(1, -1),
        window_query_weight,
        window_key_weight,
        window_value_weight,
        sink_logit.reshape(1, -1),
        gla_output_weight,
        window_output_weight,
    )[None]


def solution(mesh):
    split = Mesh(
        mesh.devices.reshape(N, N, mesh.shape["fs"], mesh.shape["tp"]), ("sp_0", "sp_1", "fs", "tp")
    )
    return jax.shard_map(
        per_device,
        mesh=split,
        in_specs=(
            P("fs", SP_TP, None), P(), P(SP, "tp"), P(SP, "tp"), P(SP, "tp"), P(SP, None),
            P(None, "tp"), P("tp"), P(), P(SP, "tp"), P(SP, "tp"), P(SP, "tp"), P("tp"),
            P("tp", SP), P("tp", SP),
        ),
        out_specs=P("fs", SP_TP, None),
        check_vma=False,
    )
```

```python
import contextlib

import jax
import jax.numpy as jnp
from jax import lax
from jax.experimental import pallas as pl
from jax.experimental.pallas import tpu as pltpu
from jax.sharding import Mesh
from jax.sharding import PartitionSpec as P

F32, BF16 = jnp.float32, jnp.bfloat16
MESH = pl.DeviceIdType.MESH
HIGH = lax.Precision.HIGHEST
SP = ("sp_0", "sp_1")
SP_TP = ("sp_0", "sp_1", "tp")
EPS = 1e-06
N = 8
SEQS = 4
D = 2048
PARTS = ((0, 5, "sp_1", "sp_0"), (5, 9, "sp_0", "sp_1"), (9, 11, "sp_1", "sp_0"), (11, 13, "sp_0", "sp_1"))


def dot(a, b, contract=((1,), (0,)), precision=None):
    return lax.dot_general(
        a, b, (contract, ((), ())), precision=precision, preferred_element_type=F32
    )


def wrap(i, n=N):
    return lax.rem(i + n, n)


def kernel(*refs):
    sources, out, places = refs[:15], refs[15], refs[16:31]
    (
        in_sems, W, T, normed, acc, kv, edge, state, got1, tot, got2, ret, enter, hid, whole, take,
        hop, hopin, fin, finin, w_send, w_line, w_far, o_line, o_far, t_send, t_recv, p_send,
        p_recv, e_sem, s_send, s_recv, o_send, o_recv, x_send, x_recv,
    ) = refs[31:]
    (
        tokens, norm_gain, gq, gk, gv, decay_down, decay_up, decay_bias, head_gain, wq, wk, wv,
        sink, go, wo,
    ) = places
    scope = contextlib.ExitStack()

    def phase(name):
        scope.close()
        scope.enter_context(jax.named_scope(name))

    phase("greet")
    z, y = lax.axis_index("sp_0"), lax.axis_index("sp_1")
    x, c = lax.axis_index("fs"), lax.axis_index("tp")
    me = z * N + y
    at = {"sp_0": z, "sp_1": y}
    right, left, across = wrap(x + 1, 4), wrap(x - 1, 4), wrap(x + 2, 4)
    partner = {"tp": 1 - c}
    after, before = wrap(me + 1, 64), wrap(me - 1, 64)
    after_id = {"sp_0": after // N, "sp_1": lax.rem(after, N)}
    before_id = {"sp_0": before // N, "sp_1": lax.rem(before, N)}

    barrier = pltpu.get_barrier_semaphore()

    def greet(device_id):
        pl.semaphore_signal(barrier, inc=1, device_id=device_id, device_id_type=MESH)

    for name in SP:
        for d in (4, 3, 5, 2, 6, 1, 7):
            greet({name: wrap(at[name] + d)})
    greet(after_id)
    greet(before_id)
    greet({"fs": right})
    greet({"fs": left})
    greet(partner)

    phase("inputs")
    for i in range(15):
        pltpu.make_async_copy(sources[i], places[i], in_sems.at[i]).start()
    for i in range(15):
        pltpu.make_async_copy(sources[i], places[i], in_sems.at[i]).wait()

    phase("pack")

    def pick(ref, width, index, count):
        got = ref[:, 0:width]
        for i in range(1, count):
            got = jnp.where(index == i, ref[:, i * width : (i + 1) * width], got)
        return got

    def put(block, value):
        W[z, y, block] = value[0:16]
        W[z, y, block + 1] = value[16:32]

    put(0, jnp.concatenate([pick(gq, 64, x, 4), pick(gk, 64, x, 4)], axis=1))
    put(2, pick(gv, 128, x, 4))
    down = decay_down[...]
    W[z, y, 4] = jnp.concatenate([down[0:16], down[16:32], jnp.zeros((16, 64), BF16)], axis=1)
    put(5, pick(wq, 128, x, 4))
    put(7, jnp.concatenate([pick(wk, 64, x // 2, 2), pick(wv, 64, x // 2, 2)], axis=1))
    put(9, pick(go, 128, x, 4))
    put(11, pick(wo, 128, x, 4))

    def norm_rows(seq, half, source=None):
        def body(q, carry):
            rows = (T[seq, half, q] if source is None else source[q]).astype(F32)
            mean_square = jnp.mean(rows * rows, axis=-1, keepdims=True)
            rows = rows * lax.rsqrt(mean_square + EPS) * norm_gain[...]
            index = (seq * 8 + half * 4 + q) * 16
            normed[pl.ds(pl.multiple_of(index, 16), 16), :] = rows.astype(BF16)
            return carry

        lax.fori_loop(0, 4, body, 0)

    norm_rows(x, c, tokens)
    phase("barrier")
    pl.semaphore_wait(barrier, 2 * (N - 1) + 5)

    def region(part, far_spot, line_spot, count):
        a, b, near, _ = PARTS[part]
        line = pl.ds(line_spot, count)
        return W.at[far_spot, line, a:b] if near == "sp_1" else W.at[line, far_spot, a:b]

    def send(part, ref, recv_sem, device_id):
        return pltpu.make_async_remote_copy(
            src_ref=ref, dst_ref=ref, send_sem=w_send.at[part], recv_sem=recv_sem,
            device_id=device_id, device_id_type=MESH,
        )

    def first_hop(part):
        _, _, near, far = PARTS[part]
        ref = region(part, at[far], at[near], 1)
        sem = w_line.at[part, at[near]] if part < 2 else o_line.at[part - 2]
        for d in (1, 7, 2, 6, 3, 5, 4):
            send(part, ref, sem, {near: wrap(at[near] + d)}).start()

    def ring_step(part, h, j):
        _, _, near, far = PARTS[part]
        up, down_ = {far: wrap(at[far] + 1)}, {far: wrap(at[far] - 1)}
        if part < 2:
            group = wrap(at[near] // 2 + (0, 1, -1, 2)[j], 4)
            count, groups, sems = 2, 4, w_far.at[part]
        else:
            group = j
            count, groups, sems = 4, 2, o_far.at[part - 2]

        def leg(far_by, device_id):
            spot = wrap(at[far] + far_by)
            return send(
                part, region(part, spot, group * count, count), sems.at[spot, group], device_id
            )

        if h == 0:
            if part < 2:
                for k in range(2):
                    spot = group * 2 + k
                    one = send(part, region(part, at[far], spot, 1), w_line.at[part, spot], up)
                    if j == 0:
                        pl.when(spot != at[near])(one.wait_recv)
                    else:
                        one.wait_recv()
            elif j == 0:
                send(part, region(part, at[far], 0, 7), o_line.at[part - 2], up).wait_recv()
            leg(0, up).start()
            leg(0, down_).start()
        elif h < 3:
            leg(-h, up).wait_recv()
            leg(-h, up).start()
            leg(h, up).wait_recv()
            leg(h, down_).start()
        elif h == 3:
            leg(-3, up).wait_recv()
            if j < groups // 2:
                leg(-3, up).start()
            leg(3, up).wait_recv()
            if j >= groups // 2:
                leg(3, down_).start()
        else:
            leg(4, up).wait_recv()

    def ring(parts, h, js):
        for j in js:
            for part in parts:
                ring_step(part, h, j)

    def chunk(seq, q, device_id, own=False):
        return pltpu.make_async_remote_copy(
            src_ref=tokens.at[q] if own else T.at[seq, c, q], dst_ref=T.at[seq, c, q],
            send_sem=t_send, recv_sem=t_recv.at[seq, q], device_id=device_id, device_id_type=MESH,
        )

    def twin(seq, q, own=False):
        return pltpu.make_async_remote_copy(
            src_ref=tokens.at[q] if own else T.at[seq, c, q], dst_ref=T.at[seq, c, q],
            send_sem=p_send, recv_sem=p_recv.at[seq], device_id=partner, device_id_type=MESH,
        )

    def tokens_step(i):
        if i < 4:
            arrivals = ((left, i, right), (right, (i + 2) % 4, left))
        else:
            arrivals = ((across, i - 4, None), (across, i - 2, None))
        for seq, q, onward in arrivals:
            chunk(seq, q, partner).wait_recv()
            if i < 2:
                chunk(seq, q, {"fs": onward}).start()
            twin(seq, q).start()

    def twins(seq):
        pltpu.make_async_remote_copy(
            src_ref=T.at[seq, 1 - c], dst_ref=T.at[seq, 1 - c], send_sem=p_send,
            recv_sem=p_recv.at[seq], device_id=partner, device_id_type=MESH,
        ).wait_recv()

    phase("first_hops")
    first_hop(0)
    first_hop(1)
    for i in range(4):
        chunk(x, i, {"fs": right}, True).start()
        chunk(x, (i + 2) % 4, {"fs": left}, True).start()
    for q in range(4):
        twin(x, q, True).start()
    phase("ring0")
    ring((0, 1), 0, (0,))
    tokens_step(0)
    ring((0, 1), 0, (1, 2))
    tokens_step(1)
    ring((0, 1), 0, (3,))
    phase("ring1")
    ring((0, 1), 1, (0,))
    tokens_step(2)
    ring((0, 1), 1, (1, 2))
    tokens_step(3)
    ring((0, 1), 1, (3,))
    phase("ring2")
    twins(x)
    norm_rows(x, 1 - c)
    ring((0, 1), 2, (0,))
    norm_rows(left, c)
    ring((0, 1), 2, (1,))
    tokens_step(4)
    norm_rows(right, c)
    ring((0, 1), 2, (2,))
    twins(left)
    norm_rows(left, 1 - c)
    tokens_step(5)
    ring((0, 1), 2, (3,))
    phase("ring3")
    twins(right)
    norm_rows(right, 1 - c)
    ring((0, 1), 3, (0,))
    norm_rows(across, c)
    ring((0, 1), 3, (1,))
    twins(across)
    norm_rows(across, 1 - c)
    ring((0, 1), 3, (2, 3))
    first_hop(2)
    first_hop(3)

    phase("proj")
    lane = lax.broadcasted_iota(jnp.int32, (N, 16, 128), 2)

    def partial(spot):
        low = W[spot, :, 4]
        zero = jnp.zeros_like(low)
        low = jnp.stack([jnp.where(lane < 32, low, zero), jnp.where(lane >= 32, low, zero)], axis=1)
        maps = [W[spot, :, 0:2], W[spot, :, 2:4], low]
        maps = jnp.concatenate([m.reshape(256, 128) for m in maps], axis=1)
        return dot(normed[:, pl.ds(pl.multiple_of(spot * 256, 256), 256)], maps)

    acc[...] = partial(z)

    def add(i, carry):
        acc[...] += partial(wrap(z + i))
        return carry

    lax.fori_loop(1, 4, add, 0)
    lax.fori_loop(5, N, add, 0)
    phase("ring4")
    ring((0,), 4, range(4))
    phase("proj_last")
    proj = acc[...] + partial(wrap(z + 4))

    def tile(block):
        return W[:, :, block : block + 2].reshape(D, 128)

    low_rank = (proj[:, 256:288] + proj[:, 288:320]).astype(BF16)
    gate = dot(low_rank, pick(decay_up, 64, x, 4)) + pick(decay_bias, 64, x, 4)
    u = jnp.exp(-jnp.abs(gate))
    log1p = jnp.where(u < 0.01, u * (1.0 - u * (0.5 - u * (1.0 / 3.0))), jnp.log(1.0 + u))
    log_rate = (jnp.minimum(gate, 0.0) - log1p) / 16.0
    query = proj[:, 0:64].astype(BF16).astype(F32) * 64**-0.5
    key = proj[:, 64:128].astype(BF16).astype(F32)
    value = proj[:, 128:256].astype(BF16).astype(F32)

    phase("update")
    lower = lax.broadcasted_iota(jnp.int32, (64, 64), 0) >= lax.broadcasted_iota(jnp.int32, (64, 64), 1)
    ones = lower.astype(F32)
    spans = [slice(64 * i, 64 * (i + 1)) for i in range(2 * SEQS)]
    within = [dot(ones, log_rate[r], precision=HIGH) for r in spans]
    totals = [w[63:64] for w in within]
    column = [jnp.transpose(jnp.broadcast_to(t, (128, 64))) for t in totals]
    update = [
        dot(jnp.transpose(key[r] * jnp.exp(t - w)), value[r], precision=HIGH)
        for r, w, t in zip(spans, within, totals)
    ]
    for seq in range(SEQS):
        a, b = 2 * seq, 2 * seq + 1
        last = jnp.exp(column[b]) * update[a] + update[b]
        fall = column[a] + column[b]
        for half in range(2):
            part = slice(32 * half, 32 * (half + 1))
            state[a + half, 0] = last[part].astype(BF16)
            state[a + half, 1] = fall[part].astype(BF16)

    def spread(stage, name, src, dst):
        place = at[name]
        for d in (4, 3, 5, 2, 6, 1, 7):
            peer = wrap(place + d)
            pltpu.make_async_remote_copy(
                src_ref=src(peer), dst_ref=dst.at[place], send_sem=s_send.at[stage],
                recv_sem=s_recv.at[stage], device_id={name: peer}, device_id_type=MESH,
            ).start()

    def spread_all(stage, dst):
        ref = dst.at[0:7]
        return pltpu.make_async_remote_copy(
            src_ref=ref, dst_ref=ref, send_sem=s_send.at[stage], recv_sem=s_recv.at[stage],
            device_id=partner, device_id_type=MESH,
        )

    phase("spread0")
    spread(0, "sp_1", lambda i: state.at[i], got1)
    got1[y] = state[y]

    phase("ring4b")
    ring((1,), 4, range(4))
    phase("wproj")
    wproj = dot(normed[...], jnp.concatenate([tile(5), tile(7)], axis=1)).astype(BF16)
    for seq in range(SEQS):
        kv[seq] = wproj[128 * seq : 128 * (seq + 1), 128:256]
    wquery = wproj[:, 0:128] * 64**-0.5
    edge_copy = pltpu.make_async_remote_copy(
        src_ref=kv, dst_ref=edge, send_sem=e_sem.at[0], recv_sem=e_sem.at[1],
        device_id=after_id, device_id_type=MESH,
    )
    phase("out_ring0")
    ring((2, 3), 0, range(2))
    edge_copy.start()
    phase("local")
    q_dec = [query[r] * jnp.exp(w) for r, w in zip(spans, within)]
    scores = [
        dot(qd, key[r] * jnp.exp(-w), ((1,), (1,)), HIGH) for r, w, qd in zip(spans, within, q_dec)
    ]
    local = [
        dot(jnp.where(lower, s, 0.0), value[r], precision=HIGH) for r, s in zip(spans, scores)
    ]

    phase("wait0")
    spread_all(0, got1).wait_recv()
    phase("scan0")
    run = jnp.zeros((32, 128), F32)
    fall = jnp.zeros((32, 128), F32)
    prefix, falls = [], []
    for i in range(N):
        prefix.append(run)
        falls.append(fall)
        step = got1[i, 1].astype(F32)
        run = jnp.exp(step) * run + got1[i, 0].astype(F32)
        fall = fall + step
    tot[0] = run.astype(BF16)
    tot[1] = fall.astype(BF16)
    spread(1, "sp_0", lambda i: tot, got2)
    got2[z] = tot[...]

    phase("out_ring1")
    ring((2, 3), 1, range(2))
    phase("edge_wait")
    edge_copy.wait()
    phase("window")
    distance = (
        lax.broadcasted_iota(jnp.int32, (128, 256), 0)
        + 128
        - lax.broadcasted_iota(jnp.int32, (128, 256), 1)
    )
    first_key = jnp.where(me > 0, 0, 128)
    valid = (distance >= 0) & (distance < 128)
    valid = valid & (lax.broadcasted_iota(jnp.int32, (128, 256), 1) >= first_key)
    sinks = pick(sink, 2, x, 4)

    def window(seqs):
        bands = [jnp.concatenate([edge[seq], kv[seq]], axis=0) for seq in seqs for _ in range(2)]
        heads = [
            (wquery[128 * seq : 128 * (seq + 1), 64 * head : 64 * (head + 1)], sinks[:, head : head + 1])
            for seq in seqs
            for head in range(2)
        ]
        s = [dot(q, band[:, 0:64], ((1,), (1,))) for (q, _), band in zip(heads, bands)]
        s = [jnp.where(valid, a, -1e30) for a in s]
        top = [jnp.maximum(jnp.max(a, axis=-1, keepdims=True), h[1]) for a, h in zip(s, heads)]
        expo = [jnp.exp(a - t) for a, t in zip(s, top)]
        denom = [
            jnp.sum(e, axis=-1, keepdims=True) + jnp.exp(h[1] - t)
            for e, t, h in zip(expo, top, heads)
        ]
        weights = [(e * (1.0 / d)).astype(BF16) for e, d in zip(expo, denom)]
        got = [dot(w, band[:, 64:128]) for w, band in zip(weights, bands)]
        for i, seq in enumerate(seqs):
            hid[seq, :, 128:256] = jnp.concatenate(got[2 * i : 2 * i + 2], axis=1).astype(BF16)

    window((0, 1))
    phase("wait1")
    spread_all(1, got2).wait_recv()
    phase("scan1")
    come = jnp.zeros((32, 128), F32)
    for i in range(N):
        come = jnp.where(
            i < z, jnp.exp(got2[i, 1].astype(F32)) * come + got2[i, 0].astype(F32), come
        )
    for i in range(N):
        ret[i] = (jnp.exp(falls[i]) * come + prefix[i]).astype(BF16)
    spread(2, "sp_1", lambda i: ret.at[i], enter)
    enter[y] = ret[y]

    phase("out_ring2")
    ring((2, 3), 2, range(2))
    phase("window2")
    window((2, 3))
    phase("out_ring3")
    ring((2, 3), 3, range(2))
    phase("wait2")
    spread_all(2, enter).wait_recv()
    phase("gla_out")
    for seq in range(SEQS):
        a, b = 2 * seq, 2 * seq + 1
        come = jnp.concatenate([enter[a], enter[b]], axis=0).astype(F32)
        middle = jnp.exp(column[a]) * come + update[a]
        for i, entering in ((a, come), (b, middle)):
            gla = local[i] + dot(q_dec[i], entering, precision=HIGH)
            mean_square = jnp.mean(gla * gla, axis=-1, keepdims=True)
            gla = gla * lax.rsqrt(mean_square + EPS) * head_gain[...]
            hid[seq, 64 * (i - a) : 64 * (i - a + 1), 0:128] = gla.astype(BF16)
    phase("out_ring4")
    ring((2, 3), 4, range(2))

    phase("out_maps")
    out_map = jnp.concatenate([tile(9), tile(11)], axis=1)

    def to_partner(seq):
        return pltpu.make_async_remote_copy(
            src_ref=whole.at[seq, 1 - c], dst_ref=take.at[seq], send_sem=o_send,
            recv_sem=o_recv.at[seq], device_id=partner, device_id_type=MESH,
        )

    def multiply(seq):
        whole[seq] = dot(hid[seq], out_map, ((1,), (1,))).astype(BF16).reshape(2, 64, D)
        to_partner(seq).start()

    def chip_sum(seq):
        to_partner(seq).wait_recv()
        return whole[seq, c].astype(F32) + take[seq].astype(F32)

    def move(index, src, dst, device_id):
        return pltpu.make_async_remote_copy(
            src_ref=src, dst_ref=dst, send_sem=x_send, recv_sem=x_recv.at[index],
            device_id={"fs": device_id}, device_id_type=MESH,
        )

    moves = [
        move(0, hop.at[0], hopin.at[0], right), move(1, hop.at[1], hopin.at[1], left),
        move(2, fin.at[1], finin.at[1], right), move(3, fin.at[2], finin.at[2], left),
        move(4, fin.at[0], finin.at[0], right), move(5, fin.at[3], finin.at[3], left),
    ]
    multiply(across)
    multiply(right)
    phase("sum_across")
    s = chip_sum(across).astype(BF16)
    hop[0] = s[:, 0:1024]
    hop[1] = s[:, 1024:2048]
    moves[0].start()
    moves[1].start()
    phase("multiply_left")
    multiply(left)
    phase("sum_right")
    to_right = chip_sum(right)
    fin[1] = to_right[:, 1024:2048].astype(BF16)
    moves[2].start()
    phase("multiply_own")
    multiply(x)
    phase("sum_left")
    to_left = chip_sum(left)
    fin[2] = to_left[:, 0:1024].astype(BF16)
    moves[3].start()
    phase("hop_right")
    moves[0].wait_recv()
    fin[0] = (to_right[:, 0:1024] + hopin[0].astype(F32)).astype(BF16)
    moves[4].start()
    phase("hop_left")
    moves[1].wait_recv()
    fin[3] = (to_left[:, 1024:2048] + hopin[1].astype(F32)).astype(BF16)
    moves[5].start()
    phase("sum_own")
    mine = chip_sum(x)
    phase("last_wait")
    for i in (2, 3, 4, 5):
        moves[i].wait_recv()
    phase("write")
    low_half = mine[:, 0:1024] + finin[0].astype(F32) + finin[2].astype(F32)
    high_half = mine[:, 1024:2048] + finin[1].astype(F32) + finin[3].astype(F32)
    out[:, 0:1024] = low_half.astype(BF16)
    out[:, 1024:2048] = high_half.astype(BF16)

    phase("drain")

    def sent(ref, sem):
        pltpu.make_async_copy(ref, ref, sem).wait()

    for part in range(4):
        a, b, _, _ = PARTS[part]
        sent(W.at[0:7, :, a:b], w_send.at[part])
        sent(W.at[0, 0:7, a:b], w_send.at[part])
    sent(T.at[0:3, 0], t_send)
    sent(T.at[0:4, 0], p_send)
    for stage, ref in enumerate((got1, got2, enter)):
        spread_all(stage, ref).wait_send()
    sent(take, o_send)
    sent(take.at[0:3], x_send)
    scope.close()


def per_device(
    tokens, norm_gain, gla_query_weight, gla_key_weight, gla_value_weight, decay_down, decay_up,
    decay_bias, head_gain, window_query_weight, window_key_weight, window_value_weight, sink_logit,
    gla_output_weight, window_output_weight,
):
    operands = (
        tokens.reshape(4, 16, D),
        norm_gain.reshape(1, D),
        gla_query_weight,
        gla_key_weight,
        gla_value_weight,
        decay_down,
        decay_up,
        decay_bias.reshape(1, -1),
        head_gain.reshape(1, -1),
        window_query_weight,
        window_key_weight,
        window_value_weight,
        sink_logit.reshape(1, -1),
        gla_output_weight.T,
        window_output_weight.T,
    )
    dma, vmem = pltpu.SemaphoreType.DMA, pltpu.VMEM
    return pl.pallas_call(
        kernel,
        out_shape=jax.ShapeDtypeStruct((64, D), BF16),
        in_specs=[pl.BlockSpec(memory_space=pltpu.HBM)] * 15,
        out_specs=pl.BlockSpec(memory_space=pltpu.VMEM),
        scratch_shapes=[vmem(a.shape, a.dtype) for a in operands]
        + [
            dma((15,)),
            vmem((N, N, 13, 16, 128), BF16),
            vmem((4, 2, 4, 16, D), BF16),
            vmem((512, D), BF16),
            vmem((512, 384), F32),
            vmem((4, 128, 128), BF16),
            vmem((4, 128, 128), BF16),
            vmem((N, 2, 32, 128), BF16),
            vmem((N, 2, 32, 128), BF16),
            vmem((2, 32, 128), BF16),
            vmem((N, 2, 32, 128), BF16),
            vmem((N, 32, 128), BF16),
            vmem((N, 32, 128), BF16),
            vmem((4, 128, 256), BF16),
            vmem((4, 2, 64, D), BF16),
            vmem((4, 64, D), BF16),
            vmem((2, 64, 1024), BF16),
            vmem((2, 64, 1024), BF16),
            vmem((4, 64, 1024), BF16),
            vmem((4, 64, 1024), BF16),
            dma((4,)),
            dma((2, N)),
            dma((2, N, 4)),
            dma((2,)),
            dma((2, N, 2)),
            dma,
            dma((4, 4)),
            dma,
            dma((4,)),
            dma((2,)),
            dma((3,)),
            dma((3,)),
            dma,
            dma((4,)),
            dma,
            dma((6,)),
        ],
        compiler_params=pltpu.CompilerParams(
            collective_id=0, has_side_effects=True, vmem_limit_bytes=48 * 1024 * 1024
        ),
    )(*[pltpu.with_memory_space_constraint(a, pltpu.HBM) for a in operands])[None]


def solution(mesh):
    split = Mesh(
        mesh.devices.reshape(N, N, mesh.shape["fs"], mesh.shape["tp"]), ("sp_0", "sp_1", "fs", "tp")
    )
    return jax.shard_map(
        per_device,
        mesh=split,
        in_specs=(
            P("fs", SP_TP, None), P(), P(SP, "tp"), P(SP, "tp"), P(SP, "tp"), P(SP, None),
            P(None, "tp"), P("tp"), P(), P(SP, "tp"), P(SP, "tp"), P(SP, "tp"), P("tp"),
            P("tp", SP), P("tp", SP),
        ),
        out_specs=P("fs", SP_TP, None),
        check_vma=False,
    )
```

```python
import contextlib

import jax
import jax.numpy as jnp
from jax import lax
from jax.experimental import pallas as pl
from jax.experimental.pallas import tpu as pltpu
from jax.sharding import Mesh
from jax.sharding import PartitionSpec as P

F32, BF16 = jnp.float32, jnp.bfloat16
MESH = pl.DeviceIdType.MESH
SP = ("sp_0", "sp_1")
SP_TP = ("sp_0", "sp_1", "tp")
EPS = 1e-06
N = 8
SEQS = 4
D = 2048
PARTS = ((0, 4, "sp_1", "sp_0"), (5, 9, "sp_0", "sp_1"), (9, 11, "sp_1", "sp_0"), (11, 13, "sp_0", "sp_1"))


def dot(a, b, contract=((1,), (0,))):
    return lax.dot_general(a, b, (contract, ((), ())), preferred_element_type=F32)


def wrap(i, n=N):
    return lax.rem(i + n, n)


def kernel(*refs):
    sources, out, places = refs[:15], refs[15], refs[16:31]
    (
        in_sems, W, T, normed, acc, low_own, low_got, l_sem, kv, edge, state, got1, tot, got2, ret, enter, hid, whole, take,
        hop, hopin, fin, finin, w_send, w_line, w_far, o_line, o_far, t_send, t_recv, p_send,
        p_recv, e_sem, s_send, s_recv, r_send, r_recv, o_send, o_recv, x_send, x_recv,
    ) = refs[31:]
    (
        tokens, norm_gain, gq, gk, gv, decay_down, decay_up, decay_bias, head_gain, wq, wk, wv,
        sink, go, wo,
    ) = places
    scope = contextlib.ExitStack()

    def phase(name):
        scope.close()
        scope.enter_context(jax.named_scope(name))

    phase("greet")
    for i in range(15):
        pltpu.make_async_copy(sources[i], places[i], in_sems.at[i]).start()
    z, y = lax.axis_index("sp_0"), lax.axis_index("sp_1")
    x, c = lax.axis_index("fs"), lax.axis_index("tp")
    me = z * N + y
    at = {"sp_0": z, "sp_1": y}
    right, left, across = wrap(x + 1, 4), wrap(x - 1, 4), wrap(x + 2, 4)
    partner = {"tp": 1 - c}
    after, before = wrap(me + 1, 64), wrap(me - 1, 64)
    after_id = {"sp_0": after // N, "sp_1": lax.rem(after, N)}
    before_id = {"sp_0": before // N, "sp_1": lax.rem(before, N)}

    barrier = pltpu.get_barrier_semaphore()

    def greet(device_id):
        pl.semaphore_signal(barrier, inc=1, device_id=device_id, device_id_type=MESH)

    for name in SP:
        for d in (4, 3, 5, 2, 6, 1, 7):
            greet({name: wrap(at[name] + d)})
    greet(after_id)
    greet(before_id)
    greet({"fs": right})
    greet({"fs": left})
    greet(partner)

    phase("inputs")
    for i in range(15):
        pltpu.make_async_copy(sources[i], places[i], in_sems.at[i]).wait()

    phase("pack")

    def pick(ref, width, index, count):
        got = ref[:, 0:width]
        for i in range(1, count):
            got = jnp.where(index == i, ref[:, i * width : (i + 1) * width], got)
        return got

    def put(block, value):
        W[z, y, block] = value[0:16]
        W[z, y, block + 1] = value[16:32]

    put(0, jnp.concatenate([pick(gq, 64, x, 4), pick(gk, 64, x, 4)], axis=1))
    put(2, pick(gv, 128, x, 4))
    down = decay_down[...]
    W[z, y, 4] = jnp.concatenate([down[0:16], down[16:32], jnp.zeros((16, 64), BF16)], axis=1)
    put(5, pick(wq, 128, x, 4))
    put(7, jnp.concatenate([pick(wk, 64, x // 2, 2), pick(wv, 64, x // 2, 2)], axis=1))
    put(9, pick(go, 128, x, 4))
    put(11, pick(wo, 128, x, 4))

    def norm_rows(seq, half, source=None):
        def body(q, carry):
            rows = (T[seq, half, q] if source is None else source[q]).astype(F32)
            mean_square = jnp.mean(rows * rows, axis=-1, keepdims=True)
            rows = rows * lax.rsqrt(mean_square + EPS) * norm_gain[...]
            index = (seq * 8 + half * 4 + q) * 16
            normed[pl.ds(pl.multiple_of(index, 16), 16), :] = rows.astype(BF16)
            return carry

        lax.fori_loop(0, 4, body, 0)

    phase("barrier")
    pl.semaphore_wait(barrier, 2 * (N - 1) + 5)

    def region(part, far_spot, line_spot, count, longer=0):
        a, b, near, _ = PARTS[part]
        b = b + longer
        line = pl.ds(line_spot, count)
        return W.at[far_spot, line, a:b] if near == "sp_1" else W.at[line, far_spot, a:b]

    def send(part, ref, recv_sem, device_id):
        return pltpu.make_async_remote_copy(
            src_ref=ref, dst_ref=ref, send_sem=w_send.at[part], recv_sem=recv_sem,
            device_id=device_id, device_id_type=MESH,
        )

    def each_core(part, act):
        if part == 0:
            pl.when(c == 0)(lambda: act(0))
            pl.when(c == 1)(lambda: act(1))
        else:
            act(0)

    def first_hop(part, by=(1, 7, 2, 6, 3, 5, 4)):
        _, _, near, far = PARTS[part]
        sem = w_line.at[part, at[near]] if part < 2 else o_line.at[part - 2]

        def act(longer):
            ref = region(part, at[far], at[near], 1, longer)
            for d in by:
                send(part, ref, sem, {near: wrap(at[near] + d)}).start()

        each_core(part, act)

    def ring_step(part, h, j):
        each_core(part, lambda longer: ring_act(part, h, j, longer))

    def ring_act(part, h, j, longer):
        _, _, near, far = PARTS[part]
        up, down_ = {far: wrap(at[far] + 1)}, {far: wrap(at[far] - 1)}
        if part < 2:
            group = wrap(at[near] // 2 + (0, 1, -1, 2)[j], 4)
            count, groups, sems = 2, 4, w_far.at[part]
        else:
            group = j
            count, groups, sems = 4, 2, o_far.at[part - 2]

        def leg(far_by, device_id):
            spot = wrap(at[far] + far_by)
            return send(
                part, region(part, spot, group * count, count, longer), sems.at[spot, group],
                device_id,
            )

        if h == 0:
            if part < 2:
                for k in range(2):
                    spot = group * 2 + k
                    one = send(
                        part, region(part, at[far], spot, 1, longer), w_line.at[part, spot], up
                    )
                    if j == 0:
                        pl.when(spot != at[near])(one.wait_recv)
                    else:
                        one.wait_recv()
            elif j == 0:
                send(part, region(part, at[far], 0, 7), o_line.at[part - 2], up).wait_recv()
            leg(0, up).start()
            leg(0, down_).start()
        elif h < 3:
            leg(-h, up).wait_recv()
            leg(-h, up).start()
            leg(h, up).wait_recv()
            leg(h, down_).start()
        elif h == 3:
            leg(-3, up).wait_recv()
            if j < groups // 2:
                leg(-3, up).start()
            leg(3, up).wait_recv()
            if j >= groups // 2:
                leg(3, down_).start()
        else:
            leg(4, up).wait_recv()

    def ring(parts, h, js):
        for j in js:
            for part in parts:
                ring_step(part, h, j)

    def chunk(seq, q, device_id, own=False):
        return pltpu.make_async_remote_copy(
            src_ref=tokens.at[q] if own else T.at[seq, c, q], dst_ref=T.at[seq, c, q],
            send_sem=t_send, recv_sem=t_recv.at[seq, q], device_id=device_id, device_id_type=MESH,
        )

    def twin(seq, q, own=False):
        return pltpu.make_async_remote_copy(
            src_ref=tokens.at[q] if own else T.at[seq, c, q], dst_ref=T.at[seq, c, q],
            send_sem=p_send, recv_sem=p_recv.at[seq], device_id=partner, device_id_type=MESH,
        )

    def tokens_step(i):
        if i < 4:
            arrivals = ((left, i, right), (right, (i + 2) % 4, left))
        else:
            arrivals = ((across, i - 4, None), (across, i - 2, None))
        for seq, q, onward in arrivals:
            chunk(seq, q, partner).wait_recv()
            if i < 2:
                chunk(seq, q, {"fs": onward}).start()
            twin(seq, q).start()

    def twins(seq):
        pltpu.make_async_remote_copy(
            src_ref=T.at[seq, 1 - c], dst_ref=T.at[seq, 1 - c], send_sem=p_send,
            recv_sem=p_recv.at[seq], device_id=partner, device_id_type=MESH,
        ).wait_recv()

    phase("first_hops")
    first_hop(0)
    first_hop(1)
    for i in range(4):
        chunk(x, i, {"fs": right}, True).start()
        chunk(x, (i + 2) % 4, {"fs": left}, True).start()
    for q in range(4):
        twin(x, q, True).start()
    norm_rows(x, c, tokens)
    phase("ring0")
    ring((0, 1), 0, (0,))
    tokens_step(0)
    ring((0, 1), 0, (1, 2))
    tokens_step(1)
    ring((0, 1), 0, (3,))
    phase("ring1")
    ring((0, 1), 1, (0,))
    tokens_step(2)
    first_hop(2, (4,))
    first_hop(3, (4,))
    ring((0, 1), 1, (1, 2))
    tokens_step(3)
    first_hop(2, (3, 5))
    first_hop(3, (3, 5))
    ring((0, 1), 1, (3,))
    phase("ring2")
    twins(x)
    norm_rows(x, 1 - c)
    ring((0, 1), 2, (0,))
    first_hop(2, (2, 6))
    first_hop(3, (2, 6))
    norm_rows(left, c)
    ring((0, 1), 2, (1,))
    first_hop(2, (1, 7))
    first_hop(3, (1, 7))
    tokens_step(4)
    norm_rows(right, c)
    ring((0, 1), 2, (2,))
    twins(left)
    norm_rows(left, 1 - c)
    tokens_step(5)
    ring((0, 1), 2, (3,))
    phase("ring3")
    twins(right)
    norm_rows(right, 1 - c)
    ring((0, 1), 3, (0,))
    norm_rows(across, c)
    ring((0, 1), 3, (1,))
    twins(across)
    norm_rows(across, 1 - c)
    ring((0, 1), 3, (2,))

    lane = lax.broadcasted_iota(jnp.int32, (N, 16, 128), 2)

    def partial(spot):
        low = W[spot, :, 4]
        zero = jnp.zeros_like(low)
        low = jnp.stack([jnp.where(lane < 32, low, zero), jnp.where(lane >= 32, low, zero)], axis=1)
        maps = [W[spot, :, 0:2], W[spot, :, 2:4], low]
        maps = jnp.concatenate([m.reshape(256, 128) for m in maps], axis=1)
        return dot(normed[:, pl.ds(pl.multiple_of(spot * 256, 256), 256)], maps)

    acc[...] = partial(z)
    ring((0, 1), 3, (3,))
    phase("out_ring0")
    ring((2, 3), 0, range(2))
    phase("proj")

    def add(i, carry):
        acc[...] += partial(wrap(z + i))
        return carry

    lax.fori_loop(1, 4, add, 0)
    lax.fori_loop(5, N, add, 0)
    phase("ring4")
    ring((0,), 4, range(4))
    phase("proj_last")
    proj = acc[...] + partial(wrap(z + 4))

    def tile(block):
        return W[:, :, block : block + 2].reshape(D, 128)

    lent = pltpu.make_async_remote_copy(
        src_ref=low_own, dst_ref=low_got, send_sem=l_sem.at[0], recv_sem=l_sem.at[1],
        device_id=partner, device_id_type=MESH,
    )
    low_rank = proj[:, 256:384]
    low_rank = (low_rank + pltpu.roll(low_rank, 96, 1)).astype(BF16)
    low_own[...] = low_rank
    pl.when(c == 1)(lent.start)
    pl.when(c == 0)(lent.wait_recv)
    low_rank = jnp.where(c == 1, low_rank, low_got[...])[:, 0:32]
    phase("out_ring1")
    ring((2, 3), 1, range(2))
    phase("gate")
    gate = dot(low_rank, pick(decay_up, 64, x, 4)) + pick(decay_bias, 64, x, 4)
    u = jnp.exp(-jnp.abs(gate))
    log1p = jnp.where(u < 0.01, u * (1.0 - u * (0.5 - u * (1.0 / 3.0))), jnp.log(1.0 + u))
    log_rate = (jnp.minimum(gate, 0.0) - log1p) / 16.0
    query = proj[:, 0:64].astype(BF16).astype(F32) * 64**-0.5
    key = proj[:, 64:128].astype(BF16).astype(F32)
    value = proj[:, 128:256].astype(BF16)

    phase("update")
    lower = lax.broadcasted_iota(jnp.int32, (64, 64), 0) >= lax.broadcasted_iota(jnp.int32, (64, 64), 1)
    ones = jnp.concatenate([lower.astype(BF16)] * 3, axis=1)
    high = log_rate.astype(BF16)
    rest = log_rate - high.astype(F32)
    middle = rest.astype(BF16)
    rest = (rest - middle.astype(F32)).astype(BF16)
    spans = [slice(64 * i, 64 * (i + 1)) for i in range(2 * SEQS)]
    within = [dot(ones, jnp.concatenate([high[r], middle[r], rest[r]], axis=0)) for r in spans]
    totals = [w[63:64] for w in within]
    column = [jnp.transpose(jnp.broadcast_to(t, (128, 64))) for t in totals]
    update = [
        dot(jnp.transpose(key[r] * jnp.exp(t - w)).astype(BF16), value[r])
        for r, w, t in zip(spans, within, totals)
    ]
    for seq in range(SEQS):
        a, b = 2 * seq, 2 * seq + 1
        last = jnp.exp(column[b]) * update[a] + update[b]
        fall = jnp.concatenate([totals[a] + totals[b], jnp.zeros((1, 64), F32)], axis=1)
        fall = jnp.broadcast_to(fall, (8, 128)).astype(BF16)
        for half in range(2):
            for k in range(4):
                at_row = 32 * half + 8 * k
                state[a + half, k] = last[at_row : at_row + 8].astype(BF16)
            state[a + half, 4] = fall

    def spread(stage, name, src, dst):
        place = at[name]
        for d in (4, 3, 5, 2, 6, 1, 7):
            peer = wrap(place + d)
            pltpu.make_async_remote_copy(
                src_ref=src(peer), dst_ref=dst.at[place], send_sem=s_send.at[stage],
                recv_sem=s_recv.at[stage], device_id={name: peer}, device_id_type=MESH,
            ).start()

    def rows_total(peer, source):
        return pltpu.make_async_remote_copy(
            src_ref=tot, dst_ref=got2.at[source], send_sem=r_send.at[peer],
            recv_sem=r_recv.at[source], device_id={"sp_0": peer}, device_id_type=MESH,
        )

    def slab(ref, i):
        return jnp.concatenate([ref[i, k] for k in range(4)], axis=0).astype(F32)

    def fall_of(row):
        turned = jnp.transpose(jnp.broadcast_to(row[:, 0:64], (128, 64)))
        return jnp.where(lax.rem(y, 2) == 0, turned[0:32], turned[32:64])

    def spread_all(stage, dst):
        ref = dst.at[0:7]
        return pltpu.make_async_remote_copy(
            src_ref=ref, dst_ref=ref, send_sem=s_send.at[stage], recv_sem=s_recv.at[stage],
            device_id=partner, device_id_type=MESH,
        )

    phase("spread0")
    spread(0, "sp_1", lambda i: state.at[i], got1)
    got1[y] = state[y]

    phase("ring4b")
    ring((1,), 4, range(4))
    phase("wproj")
    wproj = dot(normed[...], jnp.concatenate([tile(5), tile(7)], axis=1)).astype(BF16)
    for seq in range(SEQS):
        kv[seq] = wproj[128 * seq : 128 * (seq + 1), 128:256]
    wquery = wproj[:, 0:128] * 64**-0.5
    edge_copy = pltpu.make_async_remote_copy(
        src_ref=kv, dst_ref=edge, send_sem=e_sem.at[0], recv_sem=e_sem.at[1],
        device_id=after_id, device_id_type=MESH,
    )
    phase("local")
    q_dec = [(query[r] * jnp.exp(w)).astype(BF16) for r, w in zip(spans, within)]
    scores = [
        dot(qd, (key[r] * jnp.exp(-w)).astype(BF16), ((1,), (1,)))
        for r, w, qd in zip(spans, within, q_dec)
    ]
    scores = [jnp.where(lower, s, 0.0).astype(BF16) for s in scores]
    local = [dot(s, value[r]) for r, s in zip(spans, scores)]
    edge_copy.start()

    phase("out_ring2")
    ring((2, 3), 2, range(2))
    phase("wait0")
    spread_all(0, got1).wait_recv()
    phase("scan0")
    rows = [got1[i, 4].astype(F32)[0:1] for i in range(N)]
    steps = [fall_of(row) for row in rows]
    run = jnp.zeros((32, 128), F32)
    fall = jnp.zeros((32, 128), F32)
    prefix, falls = [], []
    for i in range(N):
        prefix.append(run)
        falls.append(fall)
        run = jnp.exp(steps[i]) * run + slab(got1, i)
        fall = fall + steps[i]
    for k in range(4):
        tot[k] = run[8 * k : 8 * (k + 1)].astype(BF16)
    total_row = sum(rows[1:], rows[0])
    tot[4] = jnp.broadcast_to(total_row, (8, 128)).astype(BF16)
    for d in range(1, N):
        peer = z + d
        pl.when(peer < N)(rows_total(wrap(peer), z).start)

    phase("out_ring3")
    ring((2, 3), 3, range(2))
    phase("wait1")
    for i in range(N - 1):
        pl.when(i < z)(rows_total(wrap(z + 1), i).wait_recv)
    phase("scan1")
    come = jnp.zeros((32, 128), F32)
    for i in range(N - 1):
        step = fall_of(got2[i, 4].astype(F32)[0:1])
        come = jnp.where(i < z, jnp.exp(step) * come + slab(got2, i), come)
    for i in range(N):
        ret[i] = (jnp.exp(falls[i]) * come + prefix[i]).astype(BF16)
    spread(2, "sp_1", lambda i: ret.at[i], enter)
    enter[y] = ret[y]

    phase("edge_wait")
    edge_copy.wait()
    phase("window")
    distance = (
        lax.broadcasted_iota(jnp.int32, (128, 256), 0)
        + 128
        - lax.broadcasted_iota(jnp.int32, (128, 256), 1)
    )
    first_key = jnp.where(me > 0, 0, 128)
    valid = (distance >= 0) & (distance < 128)
    valid = valid & (lax.broadcasted_iota(jnp.int32, (128, 256), 1) >= first_key)
    sinks = pick(sink, 2, x, 4)

    def window(seqs):
        bands = [jnp.concatenate([edge[seq], kv[seq]], axis=0) for seq in seqs for _ in range(2)]
        heads = [
            (wquery[128 * seq : 128 * (seq + 1), 64 * head : 64 * (head + 1)], sinks[:, head : head + 1])
            for seq in seqs
            for head in range(2)
        ]
        s = [dot(q, band[:, 0:64], ((1,), (1,))) for (q, _), band in zip(heads, bands)]
        s = [jnp.where(valid, a, -1e30) for a in s]
        top = [jnp.maximum(jnp.max(a, axis=-1, keepdims=True), h[1]) for a, h in zip(s, heads)]
        expo = [jnp.exp(a - t) for a, t in zip(s, top)]
        denom = [
            jnp.sum(e, axis=-1, keepdims=True) + jnp.exp(h[1] - t)
            for e, t, h in zip(expo, top, heads)
        ]
        weights = [(e * (1.0 / d)).astype(BF16) for e, d in zip(expo, denom)]
        got = [dot(w, band[:, 64:128]) for w, band in zip(weights, bands)]
        for i, seq in enumerate(seqs):
            hid[seq, :, 128:256] = jnp.concatenate(got[2 * i : 2 * i + 2], axis=1).astype(BF16)

    window((0, 1))
    phase("window2")
    window((2, 3))
    phase("wait2")
    spread_all(2, enter).wait_recv()
    phase("gla_out")
    for seq in range(SEQS):
        a, b = 2 * seq, 2 * seq + 1
        come = jnp.concatenate([enter[a], enter[b]], axis=0)
        middle = (jnp.exp(column[a]) * come.astype(F32) + update[a]).astype(BF16)
        for i, entering in ((a, come), (b, middle)):
            gla = local[i] + dot(q_dec[i], entering)
            mean_square = jnp.mean(gla * gla, axis=-1, keepdims=True)
            gla = gla * lax.rsqrt(mean_square + EPS) * head_gain[...]
            hid[seq, 64 * (i - a) : 64 * (i - a + 1), 0:128] = gla.astype(BF16)
    phase("out_ring4")
    ring((2, 3), 4, range(2))

    phase("out_maps")
    out_map = jnp.concatenate([tile(9), tile(11)], axis=1)

    def to_partner(seq):
        return pltpu.make_async_remote_copy(
            src_ref=whole.at[seq, 1 - c], dst_ref=take.at[seq], send_sem=o_send,
            recv_sem=o_recv.at[seq], device_id=partner, device_id_type=MESH,
        )

    def multiply(seq):
        whole[seq] = dot(hid[seq], out_map, ((1,), (1,))).astype(BF16).reshape(2, 64, D)
        to_partner(seq).start()

    def chip_sum(seq):
        to_partner(seq).wait_recv()
        return whole[seq, c].astype(F32) + take[seq].astype(F32)

    def move(index, src, dst, device_id):
        return pltpu.make_async_remote_copy(
            src_ref=src, dst_ref=dst, send_sem=x_send, recv_sem=x_recv.at[index],
            device_id={"fs": device_id}, device_id_type=MESH,
        )

    moves = [
        move(0, hop.at[0], hopin.at[0], right), move(1, hop.at[1], hopin.at[1], left),
        move(2, fin.at[1], finin.at[1], right), move(3, fin.at[2], finin.at[2], left),
        move(4, fin.at[0], finin.at[0], right), move(5, fin.at[3], finin.at[3], left),
    ]
    multiply(across)
    multiply(right)
    phase("sum_across")
    s = chip_sum(across).astype(BF16)
    hop[0] = s[:, 0:1024]
    hop[1] = s[:, 1024:2048]
    moves[0].start()
    moves[1].start()
    phase("multiply_left")
    multiply(left)
    phase("sum_right")
    to_right = chip_sum(right)
    fin[1] = to_right[:, 1024:2048].astype(BF16)
    moves[2].start()
    phase("multiply_own")
    multiply(x)
    phase("sum_left")
    to_left = chip_sum(left)
    fin[2] = to_left[:, 0:1024].astype(BF16)
    moves[3].start()
    phase("hop_right")
    moves[0].wait_recv()
    fin[0] = (to_right[:, 0:1024] + hopin[0].astype(F32)).astype(BF16)
    moves[4].start()
    phase("hop_left")
    moves[1].wait_recv()
    fin[3] = (to_left[:, 1024:2048] + hopin[1].astype(F32)).astype(BF16)
    moves[5].start()
    phase("sum_own")
    mine = chip_sum(x)
    phase("last_wait")
    for i in (2, 3, 4, 5):
        moves[i].wait_recv()
    phase("write")
    low_half = mine[:, 0:1024] + finin[0].astype(F32) + finin[2].astype(F32)
    high_half = mine[:, 1024:2048] + finin[1].astype(F32) + finin[3].astype(F32)
    out[:, 0:1024] = low_half.astype(BF16)
    out[:, 1024:2048] = high_half.astype(BF16)

    phase("drain")

    def sent(ref, sem):
        pltpu.make_async_copy(ref, ref, sem).wait()

    for part in range(4):
        a, b, _, _ = PARTS[part]

        def gone(longer):
            sent(W.at[0:7, :, a : b + longer], w_send.at[part])
            sent(W.at[0, 0:7, a : b + longer], w_send.at[part])

        each_core(part, gone)
    pl.when(c == 1)(lent.wait_send)
    sent(T.at[0:3, 0], t_send)
    sent(T.at[0:4, 0], p_send)
    spread_all(0, got1).wait_send()
    spread_all(2, enter).wait_send()
    for d in range(1, N):
        pl.when(z + d < N)(rows_total(wrap(z + d), z).wait_send)
    sent(take, o_send)
    sent(take.at[0:3], x_send)
    scope.close()


def per_device(
    tokens, norm_gain, gla_query_weight, gla_key_weight, gla_value_weight, decay_down, decay_up,
    decay_bias, head_gain, window_query_weight, window_key_weight, window_value_weight, sink_logit,
    gla_output_weight, window_output_weight,
):
    operands = (
        tokens.reshape(4, 16, D),
        norm_gain.reshape(1, D),
        gla_query_weight,
        gla_key_weight,
        gla_value_weight,
        decay_down,
        decay_up,
        decay_bias.reshape(1, -1),
        head_gain.reshape(1, -1),
        window_query_weight,
        window_key_weight,
        window_value_weight,
        sink_logit.reshape(1, -1),
        gla_output_weight.T,
        window_output_weight.T,
    )
    dma, vmem = pltpu.SemaphoreType.DMA, pltpu.VMEM
    return pl.pallas_call(
        kernel,
        out_shape=jax.ShapeDtypeStruct((64, D), BF16),
        in_specs=[pl.BlockSpec(memory_space=pltpu.HBM)] * 15,
        out_specs=pl.BlockSpec(memory_space=pltpu.VMEM),
        scratch_shapes=[vmem(a.shape, a.dtype) for a in operands]
        + [
            dma((15,)),
            vmem((N, N, 13, 16, 128), BF16),
            vmem((4, 2, 4, 16, D), BF16),
            vmem((512, D), BF16),
            vmem((512, 384), F32),
            vmem((512, 128), BF16),
            vmem((512, 128), BF16),
            dma((2,)),
            vmem((4, 128, 128), BF16),
            vmem((4, 128, 128), BF16),
            vmem((N, 5, 8, 128), BF16),
            vmem((N, 5, 8, 128), BF16),
            vmem((5, 8, 128), BF16),
            vmem((N, 5, 8, 128), BF16),
            vmem((N, 32, 128), BF16),
            vmem((N, 32, 128), BF16),
            vmem((4, 128, 256), BF16),
            vmem((4, 2, 64, D), BF16),
            vmem((4, 64, D), BF16),
            vmem((2, 64, 1024), BF16),
            vmem((2, 64, 1024), BF16),
            vmem((4, 64, 1024), BF16),
            vmem((4, 64, 1024), BF16),
            dma((4,)),
            dma((2, N)),
            dma((2, N, 4)),
            dma((2,)),
            dma((2, N, 2)),
            dma,
            dma((4, 4)),
            dma,
            dma((4,)),
            dma((2,)),
            dma((3,)),
            dma((3,)),
            dma((N,)),
            dma((N,)),
            dma,
            dma((4,)),
            dma,
            dma((6,)),
        ],
        compiler_params=pltpu.CompilerParams(
            collective_id=0, has_side_effects=True, vmem_limit_bytes=48 * 1024 * 1024
        ),
    )(*[pltpu.with_memory_space_constraint(a, pltpu.HBM) for a in operands])[None]


def solution(mesh):
    split = Mesh(
        mesh.devices.reshape(N, N, mesh.shape["fs"], mesh.shape["tp"]), ("sp_0", "sp_1", "fs", "tp")
    )
    return jax.shard_map(
        per_device,
        mesh=split,
        in_specs=(
            P("fs", SP_TP, None), P(), P(SP, "tp"), P(SP, "tp"), P(SP, "tp"), P(SP, None),
            P(None, "tp"), P("tp"), P(), P(SP, "tp"), P(SP, "tp"), P(SP, "tp"), P("tp"),
            P("tp", SP), P("tp", SP),
        ),
        out_specs=P("fs", SP_TP, None),
        check_vma=False,
    )
```

```python
import contextlib

import jax
import jax.numpy as jnp
from jax import lax
from jax.experimental import pallas as pl
from jax.experimental.pallas import tpu as pltpu
from jax.sharding import Mesh
from jax.sharding import PartitionSpec as P

F32, BF16 = jnp.float32, jnp.bfloat16
MESH = pl.DeviceIdType.MESH
HIGH = lax.Precision.HIGHEST
SP = ("sp_0", "sp_1")
SP_TP = ("sp_0", "sp_1", "tp")
EPS = 1e-06
N = 8
SEQS = 4
D = 2048
PARTS = ((0, 4, "sp_1", "sp_0"), (5, 9, "sp_0", "sp_1"), (9, 11, "sp_1", "sp_0"), (11, 13, "sp_0", "sp_1"))


def dot(a, b, contract=((1,), (0,)), precision=None):
    return lax.dot_general(
        a, b, (contract, ((), ())), precision=precision, preferred_element_type=F32
    )


def wrap(i, n=N):
    return lax.rem(i + n, n)


def kernel(*refs):
    sources, out, places = refs[:15], refs[15], refs[16:31]
    (
        in_sems, W, T, normed, acc, low_own, low_got, l_sem, kv, edge, state, got1, tot, got2, ret, enter, hid, whole, take,
        hop, hopin, fin, finin, w_send, w_line, w_far, o_line, o_far, t_send, t_recv, p_send,
        p_recv, e_sem, s_send, s_recv, r_send, r_recv, o_send, o_recv, x_send, x_recv,
    ) = refs[31:]
    (
        tokens, norm_gain, gq, gk, gv, decay_down, decay_up, decay_bias, head_gain, wq, wk, wv,
        sink, go, wo,
    ) = places
    scope = contextlib.ExitStack()

    def phase(name):
        scope.close()
        scope.enter_context(jax.named_scope(name))

    phase("greet")
    for i in range(15):
        pltpu.make_async_copy(sources[i], places[i], in_sems.at[i]).start()
    z, y = lax.axis_index("sp_0"), lax.axis_index("sp_1")
    x, c = lax.axis_index("fs"), lax.axis_index("tp")
    me = z * N + y
    at = {"sp_0": z, "sp_1": y}
    right, left, across = wrap(x + 1, 4), wrap(x - 1, 4), wrap(x + 2, 4)
    partner = {"tp": 1 - c}
    after, before = wrap(me + 1, 64), wrap(me - 1, 64)
    after_id = {"sp_0": after // N, "sp_1": lax.rem(after, N)}
    before_id = {"sp_0": before // N, "sp_1": lax.rem(before, N)}

    barrier = pltpu.get_barrier_semaphore()

    def greet(device_id):
        pl.semaphore_signal(barrier, inc=1, device_id=device_id, device_id_type=MESH)

    for name in SP:
        for d in (4, 3, 5, 2, 6, 1, 7):
            greet({name: wrap(at[name] + d)})
    greet(after_id)
    greet(before_id)
    greet({"fs": right})
    greet({"fs": left})
    greet(partner)

    phase("inputs")
    for i in range(15):
        pltpu.make_async_copy(sources[i], places[i], in_sems.at[i]).wait()

    phase("pack")

    def pick(ref, width, index, count):
        got = ref[:, 0:width]
        for i in range(1, count):
            got = jnp.where(index == i, ref[:, i * width : (i + 1) * width], got)
        return got

    def put(block, value):
        W[z, y, block] = value[0:16]
        W[z, y, block + 1] = value[16:32]

    put(0, jnp.concatenate([pick(gq, 64, x, 4), pick(gk, 64, x, 4)], axis=1))
    put(2, pick(gv, 128, x, 4))
    down = decay_down[...]
    W[z, y, 4] = jnp.concatenate([down[0:16], down[16:32], jnp.zeros((16, 64), BF16)], axis=1)
    put(5, pick(wq, 128, x, 4))
    put(7, jnp.concatenate([pick(wk, 64, x // 2, 2), pick(wv, 64, x // 2, 2)], axis=1))
    put(9, pick(go, 128, x, 4))
    put(11, pick(wo, 128, x, 4))
    for q in range(4):
        T[x, c, q] = tokens[q]

    def norm_rows():
        def body(i, carry):
            seq, half = i // 2, lax.rem(i, 2)
            rows = pl.ds(pl.multiple_of(i * 64, 64), 64)
            tiles = [slice(128 * k, 128 * (k + 1)) for k in range(D // 128)]

            def load(k):
                return T[seq, half, :, :, k].reshape(64, 128).astype(F32)

            total = jnp.zeros((64, 128), F32)
            for k in tiles:
                total = total + load(k) * load(k)
            mean_square = jnp.sum(total, axis=-1, keepdims=True) / D
            factor = lax.rsqrt(mean_square + EPS)
            for k in tiles:
                normed[rows, k] = (load(k) * factor * norm_gain[:, k]).astype(BF16)
            return carry

        lax.fori_loop(0, 2 * SEQS, body, 0)

    phase("barrier")
    pl.semaphore_wait(barrier, 2 * (N - 1) + 5)

    def region(part, far_spot, line_spot, count, longer=0):
        a, b, near, _ = PARTS[part]
        b = b + longer
        line = pl.ds(line_spot, count)
        return W.at[far_spot, line, a:b] if near == "sp_1" else W.at[line, far_spot, a:b]

    def send(part, ref, recv_sem, device_id):
        return pltpu.make_async_remote_copy(
            src_ref=ref, dst_ref=ref, send_sem=w_send.at[part], recv_sem=recv_sem,
            device_id=device_id, device_id_type=MESH,
        )

    def each_core(part, act):
        if part == 0:
            pl.when(c == 0)(lambda: act(0))
            pl.when(c == 1)(lambda: act(1))
        else:
            act(0)

    def first_hop(part, by=(1, 7, 2, 6, 3, 5, 4)):
        _, _, near, far = PARTS[part]
        sem = w_line.at[part, at[near] // 2] if part < 2 else o_line.at[part - 2]

        def act(longer):
            ref = region(part, at[far], at[near], 1, longer)
            for d in by:
                send(part, ref, sem, {near: wrap(at[near] + d)}).start()

        each_core(part, act)

    def ring_step(part, h, j):
        each_core(part, lambda longer: ring_act(part, h, j, longer))

    def ring_act(part, h, j, longer):
        _, _, near, far = PARTS[part]
        up, down_ = {far: wrap(at[far] + 1)}, {far: wrap(at[far] - 1)}
        if part < 2:
            group = wrap(at[near] // 2 + (0, 1, -1, 2)[j], 4)
            count, groups, sems = 2, 4, w_far.at[part]
        else:
            group = j
            count, groups, sems = 4, 2, o_far.at[part - 2]

        def leg(far_by, device_id):
            spot = wrap(at[far] + far_by)
            return send(
                part, region(part, spot, group * count, count, longer), sems.at[spot, group],
                device_id,
            )

        if h == 0:
            if part < 2:
                ref = region(part, at[far], group * 2, 1 if j == 0 else 2, longer)
                send(part, ref, w_line.at[part, group], up).wait_recv()
            elif j == 0:
                send(part, region(part, at[far], 0, 7), o_line.at[part - 2], up).wait_recv()
            leg(0, up).start()
            leg(0, down_).start()
        elif h < 3:
            leg(-h, up).wait_recv()
            leg(-h, up).start()
            if h == 2 and j < groups // 2:
                leg(-2, {far: wrap(at[far] + 2)}).start()
            leg(h, up).wait_recv()
            leg(h, down_).start()
            if h == 2 and j >= groups // 2:
                leg(2, {far: wrap(at[far] - 2)}).start()
        elif h == 3:
            leg(-3, up).wait_recv()
            leg(3, up).wait_recv()
        else:
            leg(4, up).wait_recv()

    def ring(parts, h, js):
        for j in js:
            for part in parts:
                ring_step(part, h, j)

    def chunk(seq, q, device_id, own=False):
        return pltpu.make_async_remote_copy(
            src_ref=tokens.at[q] if own else T.at[seq, c, q], dst_ref=T.at[seq, c, q],
            send_sem=t_send, recv_sem=t_recv.at[seq, q], device_id=device_id, device_id_type=MESH,
        )

    def twin(seq, q, own=False):
        return pltpu.make_async_remote_copy(
            src_ref=tokens.at[q] if own else T.at[seq, c, q], dst_ref=T.at[seq, c, q],
            send_sem=p_send, recv_sem=p_recv.at[seq], device_id=partner, device_id_type=MESH,
        )

    def tokens_step(i):
        if i < 4:
            arrivals = ((left, i, right), (right, (i + 2) % 4, left))
        else:
            arrivals = ((across, i - 4, None), (across, i - 2, None))
        for seq, q, onward in arrivals:
            chunk(seq, q, partner).wait_recv()
            if i < 2:
                chunk(seq, q, {"fs": onward}).start()
            twin(seq, q).start()

    def twins(seq):
        pltpu.make_async_remote_copy(
            src_ref=T.at[seq, 1 - c], dst_ref=T.at[seq, 1 - c], send_sem=p_send,
            recv_sem=p_recv.at[seq], device_id=partner, device_id_type=MESH,
        ).wait_recv()

    phase("first_hops")
    first_hop(0)
    first_hop(1)
    for i in range(4):
        chunk(x, i, {"fs": right}, True).start()
        chunk(x, (i + 2) % 4, {"fs": left}, True).start()
    for q in range(4):
        twin(x, q, True).start()
    phase("ring0")
    ring((0, 1), 0, (0,))
    tokens_step(0)
    ring((0, 1), 0, (1, 2))
    tokens_step(1)
    ring((0, 1), 0, (3,))
    phase("ring1")
    ring((0, 1), 1, (0,))
    tokens_step(2)
    first_hop(2, (4,))
    first_hop(3, (4,))
    ring((0, 1), 1, (1, 2))
    tokens_step(3)
    first_hop(2, (3, 5))
    first_hop(3, (3, 5))
    ring((0, 1), 1, (3,))
    phase("ring2")
    twins(x)
    ring((0, 1), 2, (0,))
    first_hop(2, (2, 6))
    first_hop(3, (2, 6))
    ring((0, 1), 2, (1,))
    first_hop(2, (1, 7))
    first_hop(3, (1, 7))
    tokens_step(4)
    ring((0, 1), 2, (2,))
    twins(left)
    tokens_step(5)
    ring((0, 1), 2, (3,))
    twins(right)
    twins(across)

    lane = lax.broadcasted_iota(jnp.int32, (N, 16, 128), 2)

    def partial(spot):
        low = W[spot, :, 4]
        zero = jnp.zeros_like(low)
        low = jnp.stack([jnp.where(lane < 32, low, zero), jnp.where(lane >= 32, low, zero)], axis=1)
        maps = [W[spot, :, 0:2], W[spot, :, 2:4], low]
        maps = jnp.concatenate([m.reshape(256, 128) for m in maps], axis=1)
        return dot(normed[:, pl.ds(pl.multiple_of(spot * 256, 256), 256)], maps)

    phase("norm")
    norm_rows()
    phase("proj")
    acc[...] = partial(z)

    def add(i, carry):
        acc[...] += partial(wrap(z + i))
        return carry

    lax.fori_loop(1, 3, add, 0)
    lax.fori_loop(6, N, add, 0)
    phase("out_ring0")
    ring((2, 3), 0, range(2))
    phase("ring3")
    ring((0,), 3, range(4))
    phase("proj3")
    add(3, 0)
    add(5, 0)
    phase("ring4")
    ring((0,), 4, range(4))
    phase("proj_last")
    proj = acc[...] + partial(wrap(z + 4))

    def tile(block):
        return W[:, :, block : block + 2].reshape(D, 128)

    lent = pltpu.make_async_remote_copy(
        src_ref=low_own, dst_ref=low_got, send_sem=l_sem.at[0], recv_sem=l_sem.at[1],
        device_id=partner, device_id_type=MESH,
    )
    low_rank = proj[:, 256:384]
    low_rank = (low_rank + pltpu.roll(low_rank, 96, 1)).astype(BF16)
    low_own[...] = low_rank
    pl.when(c == 1)(lent.start)
    pl.when(c == 0)(lent.wait_recv)
    low_rank = jnp.where(c == 1, low_rank, low_got[...])[:, 0:32]
    phase("gate")
    gate = dot(low_rank, pick(decay_up, 64, x, 4)) + pick(decay_bias, 64, x, 4)
    u = jnp.exp(-jnp.abs(gate))
    log1p = jnp.where(u < 0.01, u * (1.0 - u * (0.5 - u * (1.0 / 3.0))), jnp.log(1.0 + u))
    log_rate = (jnp.minimum(gate, 0.0) - log1p) / 16.0
    query = proj[:, 0:64].astype(BF16).astype(F32) * 64**-0.5
    key = proj[:, 64:128].astype(BF16).astype(F32)
    value = proj[:, 128:256].astype(BF16)

    phase("update")
    lower = lax.broadcasted_iota(jnp.int32, (64, 64), 0) >= lax.broadcasted_iota(jnp.int32, (64, 64), 1)
    ones = jnp.concatenate([lower.astype(BF16)] * 3, axis=1)
    high = log_rate.astype(BF16)
    rest = log_rate - high.astype(F32)
    middle = rest.astype(BF16)
    rest = (rest - middle.astype(F32)).astype(BF16)
    spans = [slice(64 * i, 64 * (i + 1)) for i in range(2 * SEQS)]
    within = [dot(ones, jnp.concatenate([high[r], middle[r], rest[r]], axis=0)) for r in spans]
    totals = [w[63:64] for w in within]
    column = [jnp.transpose(jnp.broadcast_to(t, (128, 64))) for t in totals]
    update = [
        dot(jnp.transpose(key[r] * jnp.exp(t - w)).astype(BF16), value[r])
        for r, w, t in zip(spans, within, totals)
    ]
    for seq in range(SEQS):
        a, b = 2 * seq, 2 * seq + 1
        last = jnp.exp(column[b]) * update[a] + update[b]
        fall = jnp.concatenate([totals[a] + totals[b], jnp.zeros((1, 64), F32)], axis=1)
        fall = jnp.broadcast_to(fall, (8, 128)).astype(BF16)
        for half in range(2):
            for k in range(4):
                at_row = 32 * half + 8 * k
                state[a + half, k] = last[at_row : at_row + 8].astype(BF16)
            state[a + half, 4] = fall

    def spread(stage, name, src, dst):
        place = at[name]
        for d in (4, 3, 5, 2, 6, 1, 7):
            peer = wrap(place + d)
            pltpu.make_async_remote_copy(
                src_ref=src(peer), dst_ref=dst.at[place], send_sem=s_send.at[stage],
                recv_sem=s_recv.at[stage], device_id={name: peer}, device_id_type=MESH,
            ).start()

    def rows_total(peer, source):
        return pltpu.make_async_remote_copy(
            src_ref=tot, dst_ref=got2.at[source], send_sem=r_send.at[peer],
            recv_sem=r_recv.at[source], device_id={"sp_0": peer}, device_id_type=MESH,
        )

    def slab(ref, i):
        return jnp.concatenate([ref[i, k] for k in range(4)], axis=0).astype(F32)

    def fall_of(row):
        turned = jnp.transpose(jnp.broadcast_to(row[:, 0:64], (128, 64)))
        return jnp.where(lax.rem(y, 2) == 0, turned[0:32], turned[32:64])

    def spread_all(stage, dst):
        ref = dst.at[0:7]
        return pltpu.make_async_remote_copy(
            src_ref=ref, dst_ref=ref, send_sem=s_send.at[stage], recv_sem=s_recv.at[stage],
            device_id=partner, device_id_type=MESH,
        )

    phase("spread0")
    spread(0, "sp_1", lambda i: state.at[i], got1)
    got1[y] = state[y]

    phase("out_ring1")
    ring((2, 3), 1, range(2))
    phase("ring4b")
    ring((1,), 3, range(4))
    ring((1,), 4, range(4))
    phase("wproj")
    wproj = dot(normed[...], jnp.concatenate([tile(5), tile(7)], axis=1)).astype(BF16)
    for seq in range(SEQS):
        kv[seq] = wproj[128 * seq : 128 * (seq + 1), 128:256]
    wquery = wproj[:, 0:128] * 64**-0.5
    edge_copy = pltpu.make_async_remote_copy(
        src_ref=kv, dst_ref=edge, send_sem=e_sem.at[0], recv_sem=e_sem.at[1],
        device_id=after_id, device_id_type=MESH,
    )
    edge_copy.start()
    phase("local")
    q_dec = [query[r] * jnp.exp(w) for r, w in zip(spans, within)]
    scores = [
        dot(qd, key[r] * jnp.exp(-w), ((1,), (1,)), HIGH)
        for r, w, qd in zip(spans, within, q_dec)
    ]
    scores = [jnp.where(lower, s, 0.0) for s in scores]
    local = [dot(s, value[r].astype(F32), precision=HIGH) for r, s in zip(spans, scores)]
    q_dec = [qd.astype(BF16) for qd in q_dec]

    phase("out_ring2")
    ring((2, 3), 2, range(2))
    phase("wait0")
    spread_all(0, got1).wait_recv()
    phase("scan0")
    rows = [got1[i, 4].astype(F32)[0:1] for i in range(N)]
    steps = [fall_of(row) for row in rows]
    run = jnp.zeros((32, 128), F32)
    fall = jnp.zeros((32, 128), F32)
    prefix, falls = [], []
    for i in range(N):
        prefix.append(run)
        falls.append(fall)
        run = jnp.exp(steps[i]) * run + slab(got1, i)
        fall = fall + steps[i]
    for k in range(4):
        tot[k] = run[8 * k : 8 * (k + 1)].astype(BF16)
    total_row = sum(rows[1:], rows[0])
    tot[4] = jnp.broadcast_to(total_row, (8, 128)).astype(BF16)
    for d in range(1, N):
        peer = z + d
        pl.when(peer < N)(rows_total(wrap(peer), z).start)

    phase("wait1")
    for i in range(N - 1):
        pl.when(i < z)(rows_total(wrap(z + 1), i).wait_recv)
    phase("scan1")
    come = jnp.zeros((32, 128), F32)
    for i in range(N - 1):
        step = fall_of(got2[i, 4].astype(F32)[0:1])
        come = jnp.where(i < z, jnp.exp(step) * come + slab(got2, i), come)
    for i in range(N):
        ret[i] = (jnp.exp(falls[i]) * come + prefix[i]).astype(BF16)
    spread(2, "sp_1", lambda i: ret.at[i], enter)
    enter[y] = ret[y]

    phase("edge_wait")
    edge_copy.wait()
    phase("window")
    distance = (
        lax.broadcasted_iota(jnp.int32, (128, 256), 0)
        + 128
        - lax.broadcasted_iota(jnp.int32, (128, 256), 1)
    )
    first_key = jnp.where(me > 0, 0, 128)
    valid = (distance >= 0) & (distance < 128)
    valid = valid & (lax.broadcasted_iota(jnp.int32, (128, 256), 1) >= first_key)
    sinks = pick(sink, 2, x, 4)

    def window(seqs):
        bands = [jnp.concatenate([edge[seq], kv[seq]], axis=0) for seq in seqs for _ in range(2)]
        heads = [
            (wquery[128 * seq : 128 * (seq + 1), 64 * head : 64 * (head + 1)], sinks[:, head : head + 1])
            for seq in seqs
            for head in range(2)
        ]
        s = [dot(q, band[:, 0:64], ((1,), (1,))) for (q, _), band in zip(heads, bands)]
        s = [jnp.where(valid, a, -1e30) for a in s]
        top = [jnp.maximum(jnp.max(a, axis=-1, keepdims=True), h[1]) for a, h in zip(s, heads)]
        expo = [jnp.exp(a - t) for a, t in zip(s, top)]
        denom = [
            jnp.sum(e, axis=-1, keepdims=True) + jnp.exp(h[1] - t)
            for e, t, h in zip(expo, top, heads)
        ]
        weights = [(e * (1.0 / d)).astype(BF16) for e, d in zip(expo, denom)]
        got = [dot(w, band[:, 64:128]) for w, band in zip(weights, bands)]
        for i, seq in enumerate(seqs):
            hid[seq, :, 128:256] = jnp.concatenate(got[2 * i : 2 * i + 2], axis=1).astype(BF16)

    window((0, 1))
    phase("window2")
    window((2, 3))
    phase("wait2")
    spread_all(2, enter).wait_recv()
    phase("gla_out")
    for seq in range(SEQS):
        a, b = 2 * seq, 2 * seq + 1
        come = jnp.concatenate([enter[a], enter[b]], axis=0)
        middle = (jnp.exp(column[a]) * come.astype(F32) + update[a]).astype(BF16)
        for i, entering in ((a, come), (b, middle)):
            gla = local[i] + dot(q_dec[i], entering)
            mean_square = jnp.mean(gla * gla, axis=-1, keepdims=True)
            gla = gla * lax.rsqrt(mean_square + EPS) * head_gain[...]
            hid[seq, 64 * (i - a) : 64 * (i - a + 1), 0:128] = gla.astype(BF16)
    phase("out_ring4")
    ring((2, 3), 3, range(2))
    ring((2, 3), 4, range(2))

    phase("out_maps")
    out_map = jnp.concatenate([tile(9), tile(11)], axis=1)

    def to_partner(seq):
        return pltpu.make_async_remote_copy(
            src_ref=whole.at[seq, 1 - c], dst_ref=take.at[seq], send_sem=o_send,
            recv_sem=o_recv.at[seq], device_id=partner, device_id_type=MESH,
        )

    def multiply(seq):
        whole[seq] = dot(hid[seq], out_map, ((1,), (1,))).astype(BF16).reshape(2, 64, D)
        to_partner(seq).start()

    def chip_sum(seq):
        to_partner(seq).wait_recv()
        return whole[seq, c].astype(F32) + take[seq].astype(F32)

    def move(index, src, dst, device_id):
        return pltpu.make_async_remote_copy(
            src_ref=src, dst_ref=dst, send_sem=x_send, recv_sem=x_recv.at[index],
            device_id={"fs": device_id}, device_id_type=MESH,
        )

    moves = [
        move(0, hop.at[0], hopin.at[0], right), move(1, hop.at[1], hopin.at[1], left),
        move(2, fin.at[1], finin.at[1], right), move(3, fin.at[2], finin.at[2], left),
        move(4, fin.at[0], finin.at[0], right), move(5, fin.at[3], finin.at[3], left),
    ]
    multiply(across)
    multiply(right)
    phase("sum_across")
    s = chip_sum(across).astype(BF16)
    hop[0] = s[:, 0:1024]
    hop[1] = s[:, 1024:2048]
    moves[0].start()
    moves[1].start()
    phase("multiply_left")
    multiply(left)
    phase("sum_right")
    to_right = chip_sum(right)
    fin[1] = to_right[:, 1024:2048].astype(BF16)
    moves[2].start()
    phase("multiply_own")
    multiply(x)
    phase("sum_left")
    to_left = chip_sum(left)
    fin[2] = to_left[:, 0:1024].astype(BF16)
    moves[3].start()
    phase("hop_right")
    moves[0].wait_recv()
    fin[0] = (to_right[:, 0:1024] + hopin[0].astype(F32)).astype(BF16)
    moves[4].start()
    phase("hop_left")
    moves[1].wait_recv()
    fin[3] = (to_left[:, 1024:2048] + hopin[1].astype(F32)).astype(BF16)
    moves[5].start()
    phase("sum_own")
    mine = chip_sum(x)
    phase("last_wait")
    for i in (2, 3, 4, 5):
        moves[i].wait_recv()
    phase("write")
    low_half = mine[:, 0:1024] + finin[0].astype(F32) + finin[2].astype(F32)
    high_half = mine[:, 1024:2048] + finin[1].astype(F32) + finin[3].astype(F32)
    out[:, 0:1024] = low_half.astype(BF16)
    out[:, 1024:2048] = high_half.astype(BF16)

    phase("drain")

    def sent(ref, sem):
        pltpu.make_async_copy(ref, ref, sem).wait()

    for part in range(4):
        a, b, _, _ = PARTS[part]

        def gone(longer):
            sent(W.at[0:7, :, a : b + longer], w_send.at[part])
            sent(W.at[0, 0:7, a : b + longer], w_send.at[part])

        each_core(part, gone)
    pl.when(c == 1)(lent.wait_send)
    sent(T.at[0:3, 0], t_send)
    sent(T.at[0:4, 0], p_send)
    spread_all(0, got1).wait_send()
    spread_all(2, enter).wait_send()
    for d in range(1, N):
        pl.when(z + d < N)(rows_total(wrap(z + d), z).wait_send)
    sent(take, o_send)
    sent(take.at[0:3], x_send)
    scope.close()


def per_device(
    tokens, norm_gain, gla_query_weight, gla_key_weight, gla_value_weight, decay_down, decay_up,
    decay_bias, head_gain, window_query_weight, window_key_weight, window_value_weight, sink_logit,
    gla_output_weight, window_output_weight,
):
    operands = (
        tokens.reshape(4, 16, D),
        norm_gain.reshape(1, D),
        gla_query_weight,
        gla_key_weight,
        gla_value_weight,
        decay_down,
        decay_up,
        decay_bias.reshape(1, -1),
        head_gain.reshape(1, -1),
        window_query_weight,
        window_key_weight,
        window_value_weight,
        sink_logit.reshape(1, -1),
        gla_output_weight.T,
        window_output_weight.T,
    )
    dma, vmem = pltpu.SemaphoreType.DMA, pltpu.VMEM
    return pl.pallas_call(
        kernel,
        out_shape=jax.ShapeDtypeStruct((64, D), BF16),
        in_specs=[pl.BlockSpec(memory_space=pltpu.HBM)] * 15,
        out_specs=pl.BlockSpec(memory_space=pltpu.VMEM),
        scratch_shapes=[vmem(a.shape, a.dtype) for a in operands]
        + [
            dma((15,)),
            vmem((N, N, 13, 16, 128), BF16),
            vmem((4, 2, 4, 16, D), BF16),
            vmem((512, D), BF16),
            vmem((512, 384), F32),
            vmem((512, 128), BF16),
            vmem((512, 128), BF16),
            dma((2,)),
            vmem((4, 128, 128), BF16),
            vmem((4, 128, 128), BF16),
            vmem((N, 5, 8, 128), BF16),
            vmem((N, 5, 8, 128), BF16),
            vmem((5, 8, 128), BF16),
            vmem((N, 5, 8, 128), BF16),
            vmem((N, 32, 128), BF16),
            vmem((N, 32, 128), BF16),
            vmem((4, 128, 256), BF16),
            vmem((4, 2, 64, D), BF16),
            vmem((4, 64, D), BF16),
            vmem((2, 64, 1024), BF16),
            vmem((2, 64, 1024), BF16),
            vmem((4, 64, 1024), BF16),
            vmem((4, 64, 1024), BF16),
            dma((4,)),
            dma((2, 4)),
            dma((2, N, 4)),
            dma((2,)),
            dma((2, N, 2)),
            dma,
            dma((4, 4)),
            dma,
            dma((4,)),
            dma((2,)),
            dma((3,)),
            dma((3,)),
            dma((N,)),
            dma((N,)),
            dma,
            dma((4,)),
            dma,
            dma((6,)),
        ],
        compiler_params=pltpu.CompilerParams(
            collective_id=0, has_side_effects=True, vmem_limit_bytes=48 * 1024 * 1024
        ),
    )(*[pltpu.with_memory_space_constraint(a, pltpu.HBM) for a in operands])[None]


def solution(mesh):
    split = Mesh(
        mesh.devices.reshape(N, N, mesh.shape["fs"], mesh.shape["tp"]), ("sp_0", "sp_1", "fs", "tp")
    )
    return jax.shard_map(
        per_device,
        mesh=split,
        in_specs=(
            P("fs", SP_TP, None), P(), P(SP, "tp"), P(SP, "tp"), P(SP, "tp"), P(SP, None),
            P(None, "tp"), P("tp"), P(), P(SP, "tp"), P(SP, "tp"), P(SP, "tp"), P("tp"),
            P("tp", SP), P("tp", SP),
        ),
        out_specs=P("fs", SP_TP, None),
        check_vma=False,
    )
```

```python
import contextlib

import jax
import jax.numpy as jnp
from jax import lax
from jax.experimental import pallas as pl
from jax.experimental.pallas import tpu as pltpu
from jax.sharding import Mesh
from jax.sharding import PartitionSpec as P

F32, BF16 = jnp.float32, jnp.bfloat16
MESH = pl.DeviceIdType.MESH
HIGH = lax.Precision.HIGHEST
SP = ("sp_0", "sp_1")
SP_TP = ("sp_0", "sp_1", "tp")
EPS = 1e-06
N = 8
SEQS = 4
D = 2048
PARTS = ((0, 4, "sp_1", "sp_0"), (5, 9, "sp_0", "sp_1"), (9, 11, "sp_1", "sp_0"), (11, 13, "sp_0", "sp_1"))


def dot(a, b, contract=((1,), (0,)), precision=None):
    return lax.dot_general(
        a, b, (contract, ((), ())), precision=precision, preferred_element_type=F32
    )


def wrap(i, n=N):
    return lax.rem(i + n, n)


def kernel(*refs):
    sources, out, places = refs[:15], refs[15], refs[16:31]
    (
        in_sems, W, T, normed, acc, low_own, low_got, l_sem, kv, edge, state, got1, tot, got2, ret, enter, hid, whole, take,
        hop, hopin, fin, finin, w_send, w_line, w_far, o_line, o_far, t_send, t_recv, p_send,
        p_recv, e_sem, s_send, s_recv, r_send, r_recv, o_send, o_recv, x_send, x_recv,
    ) = refs[31:]
    (
        tokens, norm_gain, gq, gk, gv, decay_down, decay_up, decay_bias, head_gain, wq, wk, wv,
        sink, go, wo,
    ) = places
    scope = contextlib.ExitStack()

    def phase(name):
        scope.close()
        scope.enter_context(jax.named_scope(name))

    phase("greet")
    for i in range(15):
        pltpu.make_async_copy(sources[i], places[i], in_sems.at[i]).start()
    z, y = lax.axis_index("sp_0"), lax.axis_index("sp_1")
    x, c = lax.axis_index("fs"), lax.axis_index("tp")
    me = z * N + y
    at = {"sp_0": z, "sp_1": y}
    right, left, across = wrap(x + 1, 4), wrap(x - 1, 4), wrap(x + 2, 4)
    partner = {"tp": 1 - c}
    after, before = wrap(me + 1, 64), wrap(me - 1, 64)
    after_id = {"sp_0": after // N, "sp_1": lax.rem(after, N)}
    before_id = {"sp_0": before // N, "sp_1": lax.rem(before, N)}

    barrier = pltpu.get_barrier_semaphore()

    def greet(device_id):
        pl.semaphore_signal(barrier, inc=1, device_id=device_id, device_id_type=MESH)

    for name in SP:
        for d in (4, 3, 5, 2, 6, 1, 7):
            greet({name: wrap(at[name] + d)})
    greet(after_id)
    greet(before_id)
    greet({"fs": right})
    greet({"fs": left})
    greet(partner)

    phase("inputs")
    for i in range(15):
        pltpu.make_async_copy(sources[i], places[i], in_sems.at[i]).wait()

    phase("pack")

    def pick(ref, width, index, count):
        got = ref[:, 0:width]
        for i in range(1, count):
            got = jnp.where(index == i, ref[:, i * width : (i + 1) * width], got)
        return got

    def put(block, value):
        W[z, y, block] = value[0:16]
        W[z, y, block + 1] = value[16:32]

    put(0, jnp.concatenate([pick(gq, 64, x, 4), pick(gk, 64, x, 4)], axis=1))
    put(2, pick(gv, 128, x, 4))
    down = decay_down[...]
    W[z, y, 4] = jnp.concatenate([down[0:16], down[16:32], jnp.zeros((16, 64), BF16)], axis=1)
    put(5, pick(wq, 128, x, 4))
    put(7, jnp.concatenate([pick(wk, 64, x // 2, 2), pick(wv, 64, x // 2, 2)], axis=1))
    put(9, pick(go, 128, x, 4))
    put(11, pick(wo, 128, x, 4))
    for q in range(4):
        T[x, c, q] = tokens[q]

    def norm_rows():
        def body(i, carry):
            seq, half = i // 2, lax.rem(i, 2)
            rows = pl.ds(pl.multiple_of(i * 64, 64), 64)
            tiles = [slice(128 * k, 128 * (k + 1)) for k in range(D // 128)]

            def load(k):
                return T[seq, half, :, :, k].reshape(64, 128).astype(F32)

            total = jnp.zeros((64, 128), F32)
            for k in tiles:
                total = total + load(k) * load(k)
            mean_square = jnp.sum(total, axis=-1, keepdims=True) / D
            factor = lax.rsqrt(mean_square + EPS)
            for k in tiles:
                normed[rows, k] = (load(k) * factor * norm_gain[:, k]).astype(BF16)
            return carry

        lax.fori_loop(0, 2 * SEQS, body, 0)

    phase("barrier")
    pl.semaphore_wait(barrier, 2 * (N - 1) + 5)

    def region(part, far_spot, line_spot, count, longer=0):
        a, b, near, _ = PARTS[part]
        b = b + longer
        line = pl.ds(line_spot, count)
        return W.at[far_spot, line, a:b] if near == "sp_1" else W.at[line, far_spot, a:b]

    def send(part, ref, recv_sem, device_id):
        return pltpu.make_async_remote_copy(
            src_ref=ref, dst_ref=ref, send_sem=w_send.at[part], recv_sem=recv_sem,
            device_id=device_id, device_id_type=MESH,
        )

    def each_core(part, act):
        if part == 0:
            pl.when(c == 0)(lambda: act(0))
            pl.when(c == 1)(lambda: act(1))
        else:
            act(0)

    def first_hop(part, by=(1, 7, 2, 6, 3, 5, 4)):
        _, _, near, far = PARTS[part]
        sem = w_line.at[part, at[near] // 2] if part < 2 else o_line.at[part - 2]

        def act(longer):
            ref = region(part, at[far], at[near], 1, longer)
            for d in by:
                send(part, ref, sem, {near: wrap(at[near] + d)}).start()

        each_core(part, act)

    def ring_step(part, h, j):
        each_core(part, lambda longer: ring_act(part, h, j, longer))

    def ring_act(part, h, j, longer):
        _, _, near, far = PARTS[part]
        up, down_ = {far: wrap(at[far] + 1)}, {far: wrap(at[far] - 1)}
        if part < 2:
            group = wrap(at[near] // 2 + (0, 1, -1, 2)[j], 4)
            count, groups, sems = 2, 4, w_far.at[part]
        else:
            group = j
            count, groups, sems = 4, 2, o_far.at[part - 2]

        def leg(far_by, device_id):
            spot = wrap(at[far] + far_by)
            return send(
                part, region(part, spot, group * count, count, longer), sems.at[spot, group],
                device_id,
            )

        if h == 0:
            if part < 2:
                ref = region(part, at[far], group * 2, 1 if j == 0 else 2, longer)
                send(part, ref, w_line.at[part, group], up).wait_recv()
            elif j == 0:
                send(part, region(part, at[far], 0, 7), o_line.at[part - 2], up).wait_recv()
            leg(0, up).start()
            leg(0, down_).start()
        elif h < 3:
            leg(-h, up).wait_recv()
            leg(-h, up).start()
            if h == 2 and j < groups // 2:
                leg(-2, {far: wrap(at[far] + 2)}).start()
            leg(h, up).wait_recv()
            leg(h, down_).start()
            if h == 2 and j >= groups // 2:
                leg(2, {far: wrap(at[far] - 2)}).start()
        elif h == 3:
            leg(-3, up).wait_recv()
            leg(3, up).wait_recv()
        else:
            leg(4, up).wait_recv()

    def ring(parts, h, js):
        for j in js:
            for part in parts:
                ring_step(part, h, j)

    def chunk(seq, q, device_id, own=False):
        return pltpu.make_async_remote_copy(
            src_ref=tokens.at[q] if own else T.at[seq, c, q], dst_ref=T.at[seq, c, q],
            send_sem=t_send, recv_sem=t_recv.at[seq, q], device_id=device_id, device_id_type=MESH,
        )

    def twin(seq, q, own=False):
        return pltpu.make_async_remote_copy(
            src_ref=tokens.at[q] if own else T.at[seq, c, q], dst_ref=T.at[seq, c, q],
            send_sem=p_send, recv_sem=p_recv.at[seq], device_id=partner, device_id_type=MESH,
        )

    def tokens_step(i):
        if i < 4:
            arrivals = ((left, i, right), (right, (i + 2) % 4, left))
        else:
            arrivals = ((across, i - 4, None), (across, i - 2, None))
        for seq, q, onward in arrivals:
            chunk(seq, q, partner).wait_recv()
            if i < 2:
                chunk(seq, q, {"fs": onward}).start()
            twin(seq, q).start()

    def twins(seq):
        pltpu.make_async_remote_copy(
            src_ref=T.at[seq, 1 - c], dst_ref=T.at[seq, 1 - c], send_sem=p_send,
            recv_sem=p_recv.at[seq], device_id=partner, device_id_type=MESH,
        ).wait_recv()

    phase("first_hops")
    first_hop(0)
    first_hop(1)
    for i in range(4):
        chunk(x, i, {"fs": right}, True).start()
        chunk(x, (i + 2) % 4, {"fs": left}, True).start()
    for q in range(4):
        twin(x, q, True).start()
    phase("ring0")
    ring((0, 1), 0, range(4))
    tokens_step(0)
    tokens_step(1)
    phase("ring1")
    ring((0, 1), 1, (0,))
    tokens_step(2)
    first_hop(2, (4,))
    first_hop(3, (4,))
    ring((0, 1), 1, (1, 2))
    first_hop(2, (3, 5))
    first_hop(3, (3, 5))
    ring((0, 1), 1, (3,))
    tokens_step(3)
    phase("ring2")
    twins(x)
    ring((0, 1), 2, (0,))
    first_hop(2, (2, 6))
    first_hop(3, (2, 6))
    ring((0, 1), 2, (1,))
    first_hop(2, (1, 7))
    first_hop(3, (1, 7))
    tokens_step(4)
    ring((0, 1), 2, (2, 3))
    tokens_step(5)
    twins(left)
    twins(right)
    twins(across)

    lane = lax.broadcasted_iota(jnp.int32, (N, 16, 128), 2)

    def partial(spot):
        low = W[spot, :, 4]
        zero = jnp.zeros_like(low)
        low = jnp.stack([jnp.where(lane < 32, low, zero), jnp.where(lane >= 32, low, zero)], axis=1)
        maps = [W[spot, :, 0:2], W[spot, :, 2:4], low]
        maps = jnp.concatenate([m.reshape(256, 128) for m in maps], axis=1)
        return dot(normed[:, pl.ds(pl.multiple_of(spot * 256, 256), 256)], maps)

    phase("norm")
    norm_rows()
    phase("proj")
    acc[...] = partial(z)

    def add(i, carry):
        acc[...] += partial(wrap(z + i))
        return carry

    lax.fori_loop(1, 3, add, 0)
    lax.fori_loop(6, N, add, 0)
    phase("out_ring0")
    ring((2, 3), 0, range(2))
    phase("ring3")
    ring((0,), 3, range(4))
    phase("proj3")
    add(3, 0)
    add(5, 0)
    phase("ring4")
    ring((0,), 4, range(4))
    phase("proj_last")
    proj = acc[...] + partial(wrap(z + 4))

    def tile(block):
        return W[:, :, block : block + 2].reshape(D, 128)

    lent = pltpu.make_async_remote_copy(
        src_ref=low_own, dst_ref=low_got, send_sem=l_sem.at[0], recv_sem=l_sem.at[1],
        device_id=partner, device_id_type=MESH,
    )
    low_rank = proj[:, 256:384]
    low_rank = (low_rank + pltpu.roll(low_rank, 96, 1)).astype(BF16)
    low_own[...] = low_rank
    pl.when(c == 1)(lent.start)
    pl.when(c == 0)(lent.wait_recv)
    low_rank = jnp.where(c == 1, low_rank, low_got[...])[:, 0:32]
    phase("gate")
    gate = dot(low_rank, pick(decay_up, 64, x, 4)) + pick(decay_bias, 64, x, 4)
    u = jnp.exp(-jnp.abs(gate))
    log1p = jnp.where(u < 0.01, u * (1.0 - u * (0.5 - u * (1.0 / 3.0))), jnp.log(1.0 + u))
    log_rate = (jnp.minimum(gate, 0.0) - log1p) / 16.0
    query = proj[:, 0:64].astype(BF16).astype(F32) * 64**-0.5
    key = proj[:, 64:128].astype(BF16).astype(F32)
    value = proj[:, 128:256].astype(BF16)

    phase("update")
    lower = lax.broadcasted_iota(jnp.int32, (64, 64), 0) >= lax.broadcasted_iota(jnp.int32, (64, 64), 1)
    ones = jnp.concatenate([lower.astype(BF16)] * 3, axis=1)
    high = log_rate.astype(BF16)
    rest = log_rate - high.astype(F32)
    middle = rest.astype(BF16)
    rest = (rest - middle.astype(F32)).astype(BF16)
    spans = [slice(64 * i, 64 * (i + 1)) for i in range(2 * SEQS)]
    within = [dot(ones, jnp.concatenate([high[r], middle[r], rest[r]], axis=0)) for r in spans]
    totals = [w[63:64] for w in within]
    column = [jnp.transpose(jnp.broadcast_to(t, (128, 64))) for t in totals]
    update = [
        dot(jnp.transpose(key[r] * jnp.exp(t - w)).astype(BF16), value[r])
        for r, w, t in zip(spans, within, totals)
    ]
    for seq in range(SEQS):
        a, b = 2 * seq, 2 * seq + 1
        last = jnp.exp(column[b]) * update[a] + update[b]
        fall = jnp.concatenate([totals[a] + totals[b], jnp.zeros((1, 64), F32)], axis=1)
        fall = jnp.broadcast_to(fall, (8, 128)).astype(BF16)
        for half in range(2):
            for k in range(4):
                at_row = 32 * half + 8 * k
                state[a + half, k] = last[at_row : at_row + 8].astype(BF16)
            state[a + half, 4] = fall

    def spread(stage, name, src, dst):
        place = at[name]
        for d in (4, 3, 5, 2, 6, 1, 7):
            peer = wrap(place + d)
            pltpu.make_async_remote_copy(
                src_ref=src(peer), dst_ref=dst.at[place], send_sem=s_send.at[stage],
                recv_sem=s_recv.at[stage], device_id={name: peer}, device_id_type=MESH,
            ).start()

    def rows_total(peer, source):
        return pltpu.make_async_remote_copy(
            src_ref=tot, dst_ref=got2.at[source], send_sem=r_send.at[peer],
            recv_sem=r_recv.at[source], device_id={"sp_0": peer}, device_id_type=MESH,
        )

    def slab(ref, i):
        return jnp.concatenate([ref[i, k] for k in range(4)], axis=0).astype(F32)

    def fall_of(row):
        turned = jnp.transpose(jnp.broadcast_to(row[:, 0:64], (128, 64)))
        return jnp.where(lax.rem(y, 2) == 0, turned[0:32], turned[32:64])

    def spread_all(stage, dst):
        ref = dst.at[0:7]
        return pltpu.make_async_remote_copy(
            src_ref=ref, dst_ref=ref, send_sem=s_send.at[stage], recv_sem=s_recv.at[stage],
            device_id=partner, device_id_type=MESH,
        )

    phase("spread0")
    spread(0, "sp_1", lambda i: state.at[i], got1)
    got1[y] = state[y]

    phase("out_ring1")
    ring((2, 3), 1, range(2))
    phase("ring4b")
    ring((1,), 3, range(4))
    ring((1,), 4, range(4))
    phase("wproj")
    wproj = dot(normed[...], jnp.concatenate([tile(5), tile(7)], axis=1)).astype(BF16)
    for seq in range(SEQS):
        kv[seq] = wproj[128 * seq : 128 * (seq + 1), 128:256]
    wquery = wproj[:, 0:128] * 64**-0.5
    edge_copy = pltpu.make_async_remote_copy(
        src_ref=kv, dst_ref=edge, send_sem=e_sem.at[0], recv_sem=e_sem.at[1],
        device_id=after_id, device_id_type=MESH,
    )
    edge_copy.start()
    phase("local")
    q_dec = [query[r] * jnp.exp(w) for r, w in zip(spans, within)]
    scores = [
        dot(qd, key[r] * jnp.exp(-w), ((1,), (1,)), HIGH)
        for r, w, qd in zip(spans, within, q_dec)
    ]
    scores = [jnp.where(lower, s, 0.0) for s in scores]
    local = [dot(s, value[r].astype(F32), precision=HIGH) for r, s in zip(spans, scores)]
    q_dec = [qd.astype(BF16) for qd in q_dec]

    phase("out_ring2")
    ring((2, 3), 2, range(2))
    phase("wait0")
    spread_all(0, got1).wait_recv()
    phase("scan0")
    rows = [got1[i, 4].astype(F32)[0:1] for i in range(N)]
    steps = [fall_of(row) for row in rows]
    run = jnp.zeros((32, 128), F32)
    fall = jnp.zeros((32, 128), F32)
    prefix, falls = [], []
    for i in range(N):
        prefix.append(run)
        falls.append(fall)
        run = jnp.exp(steps[i]) * run + slab(got1, i)
        fall = fall + steps[i]
    for k in range(4):
        tot[k] = run[8 * k : 8 * (k + 1)].astype(BF16)
    total_row = sum(rows[1:], rows[0])
    tot[4] = jnp.broadcast_to(total_row, (8, 128)).astype(BF16)
    for d in range(1, N):
        peer = z + d
        pl.when(peer < N)(rows_total(wrap(peer), z).start)

    phase("wait1")
    for i in range(N - 1):
        pl.when(i < z)(rows_total(wrap(z + 1), i).wait_recv)
    phase("scan1")
    come = jnp.zeros((32, 128), F32)
    for i in range(N - 1):
        step = fall_of(got2[i, 4].astype(F32)[0:1])
        come = jnp.where(i < z, jnp.exp(step) * come + slab(got2, i), come)
    for i in range(N):
        ret[i] = (jnp.exp(falls[i]) * come + prefix[i]).astype(BF16)
    spread(2, "sp_1", lambda i: ret.at[i], enter)
    enter[y] = ret[y]

    phase("edge_wait")
    edge_copy.wait()
    phase("window")
    distance = (
        lax.broadcasted_iota(jnp.int32, (128, 256), 0)
        + 128
        - lax.broadcasted_iota(jnp.int32, (128, 256), 1)
    )
    first_key = jnp.where(me > 0, 0, 128)
    valid = (distance >= 0) & (distance < 128)
    valid = valid & (lax.broadcasted_iota(jnp.int32, (128, 256), 1) >= first_key)
    sinks = pick(sink, 2, x, 4)

    def window(seqs):
        bands = [jnp.concatenate([edge[seq], kv[seq]], axis=0) for seq in seqs for _ in range(2)]
        heads = [
            (wquery[128 * seq : 128 * (seq + 1), 64 * head : 64 * (head + 1)], sinks[:, head : head + 1])
            for seq in seqs
            for head in range(2)
        ]
        s = [dot(q, band[:, 0:64], ((1,), (1,))) for (q, _), band in zip(heads, bands)]
        s = [jnp.where(valid, a, -1e30) for a in s]
        top = [jnp.maximum(jnp.max(a, axis=-1, keepdims=True), h[1]) for a, h in zip(s, heads)]
        expo = [jnp.exp(a - t) for a, t in zip(s, top)]
        denom = [
            jnp.sum(e, axis=-1, keepdims=True) + jnp.exp(h[1] - t)
            for e, t, h in zip(expo, top, heads)
        ]
        weights = [(e * (1.0 / d)).astype(BF16) for e, d in zip(expo, denom)]
        got = [dot(w, band[:, 64:128]) for w, band in zip(weights, bands)]
        for i, seq in enumerate(seqs):
            hid[seq, :, 128:256] = jnp.concatenate(got[2 * i : 2 * i + 2], axis=1).astype(BF16)

    window((0, 1))
    phase("window2")
    window((2, 3))
    phase("wait2")
    spread_all(2, enter).wait_recv()
    phase("gla_out")
    for seq in range(SEQS):
        a, b = 2 * seq, 2 * seq + 1
        come = jnp.concatenate([enter[a], enter[b]], axis=0)
        middle = (jnp.exp(column[a]) * come.astype(F32) + update[a]).astype(BF16)
        for i, entering in ((a, come), (b, middle)):
            gla = local[i] + dot(q_dec[i], entering)
            mean_square = jnp.mean(gla * gla, axis=-1, keepdims=True)
            gla = gla * lax.rsqrt(mean_square + EPS) * head_gain[...]
            hid[seq, 64 * (i - a) : 64 * (i - a + 1), 0:128] = gla.astype(BF16)
    phase("out_ring4")
    ring((2, 3), 3, range(2))
    ring((2, 3), 4, range(2))

    phase("out_maps")
    out_map = jnp.concatenate([tile(9), tile(11)], axis=1)

    def to_partner(seq):
        return pltpu.make_async_remote_copy(
            src_ref=whole.at[seq, 1 - c], dst_ref=take.at[seq], send_sem=o_send,
            recv_sem=o_recv.at[seq], device_id=partner, device_id_type=MESH,
        )

    def multiply(seq):
        whole[seq] = dot(hid[seq], out_map, ((1,), (1,))).astype(BF16).reshape(2, 64, D)
        to_partner(seq).start()

    def chip_sum(seq):
        to_partner(seq).wait_recv()
        return whole[seq, c].astype(F32) + take[seq].astype(F32)

    def move(index, src, dst, device_id):
        return pltpu.make_async_remote_copy(
            src_ref=src, dst_ref=dst, send_sem=x_send, recv_sem=x_recv.at[index],
            device_id={"fs": device_id}, device_id_type=MESH,
        )

    moves = [
        move(0, hop.at[0], hopin.at[0], right), move(1, hop.at[1], hopin.at[1], left),
        move(2, fin.at[1], finin.at[1], right), move(3, fin.at[2], finin.at[2], left),
        move(4, fin.at[0], finin.at[0], right), move(5, fin.at[3], finin.at[3], left),
    ]
    multiply(across)
    multiply(right)
    phase("sum_across")
    s = chip_sum(across).astype(BF16)
    hop[0] = s[:, 0:1024]
    hop[1] = s[:, 1024:2048]
    moves[0].start()
    moves[1].start()
    phase("multiply_left")
    multiply(left)
    phase("sum_right")
    to_right = chip_sum(right)
    fin[1] = to_right[:, 1024:2048].astype(BF16)
    moves[2].start()
    phase("multiply_own")
    multiply(x)
    phase("sum_left")
    to_left = chip_sum(left)
    fin[2] = to_left[:, 0:1024].astype(BF16)
    moves[3].start()
    phase("hop_right")
    moves[0].wait_recv()
    fin[0] = (to_right[:, 0:1024] + hopin[0].astype(F32)).astype(BF16)
    moves[4].start()
    phase("hop_left")
    moves[1].wait_recv()
    fin[3] = (to_left[:, 1024:2048] + hopin[1].astype(F32)).astype(BF16)
    moves[5].start()
    phase("sum_own")
    mine = chip_sum(x)
    phase("last_wait")
    for i in (2, 3, 4, 5):
        moves[i].wait_recv()
    phase("write")
    low_half = mine[:, 0:1024] + finin[0].astype(F32) + finin[2].astype(F32)
    high_half = mine[:, 1024:2048] + finin[1].astype(F32) + finin[3].astype(F32)
    out[:, 0:1024] = low_half.astype(BF16)
    out[:, 1024:2048] = high_half.astype(BF16)

    phase("drain")

    def sent(ref, sem):
        pltpu.make_async_copy(ref, ref, sem).wait()

    for part in range(4):
        a, b, _, _ = PARTS[part]

        def gone(longer):
            sent(W.at[0:7, :, a : b + longer], w_send.at[part])
            sent(W.at[0, 0:7, a : b + longer], w_send.at[part])

        each_core(part, gone)
    pl.when(c == 1)(lent.wait_send)
    sent(T.at[0:3, 0], t_send)
    sent(T.at[0:4, 0], p_send)
    spread_all(0, got1).wait_send()
    spread_all(2, enter).wait_send()
    for d in range(1, N):
        pl.when(z + d < N)(rows_total(wrap(z + d), z).wait_send)
    sent(take, o_send)
    sent(take.at[0:3], x_send)
    scope.close()


def per_device(
    tokens, norm_gain, gla_query_weight, gla_key_weight, gla_value_weight, decay_down, decay_up,
    decay_bias, head_gain, window_query_weight, window_key_weight, window_value_weight, sink_logit,
    gla_output_weight, window_output_weight,
):
    operands = (
        tokens.reshape(4, 16, D),
        norm_gain.reshape(1, D),
        gla_query_weight,
        gla_key_weight,
        gla_value_weight,
        decay_down,
        decay_up,
        decay_bias.reshape(1, -1),
        head_gain.reshape(1, -1),
        window_query_weight,
        window_key_weight,
        window_value_weight,
        sink_logit.reshape(1, -1),
        gla_output_weight.T,
        window_output_weight.T,
    )
    dma, vmem = pltpu.SemaphoreType.DMA, pltpu.VMEM
    return pl.pallas_call(
        kernel,
        out_shape=jax.ShapeDtypeStruct((64, D), BF16),
        in_specs=[pl.BlockSpec(memory_space=pltpu.HBM)] * 15,
        out_specs=pl.BlockSpec(memory_space=pltpu.VMEM),
        scratch_shapes=[vmem(a.shape, a.dtype) for a in operands]
        + [
            dma((15,)),
            vmem((N, N, 13, 16, 128), BF16),
            vmem((4, 2, 4, 16, D), BF16),
            vmem((512, D), BF16),
            vmem((512, 384), F32),
            vmem((512, 128), BF16),
            vmem((512, 128), BF16),
            dma((2,)),
            vmem((4, 128, 128), BF16),
            vmem((4, 128, 128), BF16),
            vmem((N, 5, 8, 128), BF16),
            vmem((N, 5, 8, 128), BF16),
            vmem((5, 8, 128), BF16),
            vmem((N, 5, 8, 128), BF16),
            vmem((N, 32, 128), BF16),
            vmem((N, 32, 128), BF16),
            vmem((4, 128, 256), BF16),
            vmem((4, 2, 64, D), BF16),
            vmem((4, 64, D), BF16),
            vmem((2, 64, 1024), BF16),
            vmem((2, 64, 1024), BF16),
            vmem((4, 64, 1024), BF16),
            vmem((4, 64, 1024), BF16),
            dma((4,)),
            dma((2, 4)),
            dma((2, N, 4)),
            dma((2,)),
            dma((2, N, 2)),
            dma,
            dma((4, 4)),
            dma,
            dma((4,)),
            dma((2,)),
            dma((3,)),
            dma((3,)),
            dma((N,)),
            dma((N,)),
            dma,
            dma((4,)),
            dma,
            dma((6,)),
        ],
        compiler_params=pltpu.CompilerParams(
            collective_id=0, has_side_effects=True, vmem_limit_bytes=48 * 1024 * 1024
        ),
    )(*[pltpu.with_memory_space_constraint(a, pltpu.HBM) for a in operands])[None]


def solution(mesh):
    split = Mesh(
        mesh.devices.reshape(N, N, mesh.shape["fs"], mesh.shape["tp"]), ("sp_0", "sp_1", "fs", "tp")
    )
    return jax.shard_map(
        per_device,
        mesh=split,
        in_specs=(
            P("fs", SP_TP, None), P(), P(SP, "tp"), P(SP, "tp"), P(SP, "tp"), P(SP, None),
            P(None, "tp"), P("tp"), P(), P(SP, "tp"), P(SP, "tp"), P(SP, "tp"), P("tp"),
            P("tp", SP), P("tp", SP),
        ),
        out_specs=P("fs", SP_TP, None),
        check_vma=False,
    )
```
